32 devices in a mesh: gr: 2 (over x), sp: 8 (over z, y), tp: 2 (over core).
Axes of the slice: x: 2, y: 2, z: 4, core: 2. Of those that a mesh axis runs over, the one named last changes fastest.
Arguments:
- tokens: bfloat16 [4, 2, 2048, 4096], P('gr', 'tp', 'sp'), may hold values from -6 to 6
- ln_gain: bfloat16 [4096], replicated, may hold values from 0.099609375 to 1.8984375
- w_key: bfloat16 [4096, 256], P('sp'), may hold values from -0.09375 to 0.09375
- w_value: bfloat16 [4096, 256], P('sp'), may hold values from -0.09375 to 0.09375
- queries: bfloat16 [16, 512], P(('gr', 'sp')), may hold values from -6 to 6
- head_shift: float32 [4, 8], replicated
- key_shift: float32 [16, 4096], P(('gr', 'sp'), 'tp')
Outputs:
- kv_cache: bfloat16 [16, 4096, 128], P(('gr', 'sp'), 'tp')
- first_read: float32 [16, 512], P(('gr', 'sp'))
The draws below stay inside these ranges and needn't reach their ends.
All inputs are finite; a program needn't handle non-finite values.
Results may differ from the reference program's by a relative error of at most 0.0064.
Values may be sent and summed in bfloat16 or wider, within the bound.
A program may use at most 64 MiB of HBM per device.

```python
import math
import jax
import jax.numpy as jnp
from jax import lax

D = 4096
HD = 64
KVH = 4
GROUP = 8
SEQS = 4
SECTIONS = 2
SPAN = 2048
LEN = 4096
PAIRS = 16


def draw_head_shift(key, part):
    first, second, third = jax.random.split(key, 3)
    fast_share = 0.5
    picker = jax.random.uniform(first, (KVH, GROUP), jnp.float32)
    fast_value = jax.random.uniform(second, (KVH, GROUP), jnp.float32, -4.5, -3.5)
    slow_value = -math.log(LEN) - 1.5 + jax.random.uniform(third, (KVH, GROUP), jnp.float32, -0.3, 0.3)
    return jnp.where(picker < fast_share, fast_value, slow_value)


def draw_key_shift(key, part):
    first, second, third, fourth = jax.random.split(key, 4)
    spread = 0.7
    section_level = jax.random.uniform(first, (PAIRS, SECTIONS), jnp.float32, -spread, spread)
    section_full = jnp.repeat(section_level, SPAN, axis=1)
    rough = jax.random.uniform(second, (PAIRS, LEN), jnp.float32, -0.5, 0.5)
    places = jax.random.randint(third, (PAIRS, 4), 0, LEN)
    marks = jnp.any(jnp.arange(LEN)[None, None, :] == places[:, :, None], axis=1)
    height = math.log(LEN) + 0.5 + jax.random.uniform(fourth, (PAIRS, LEN), jnp.float32, -0.3, 0.3)
    return section_full + rough + jnp.where(marks, height, 0.0)


def levels(key, extent, cuts, smallest, top_value):
    level = 1.0
    for dim, blocks in cuts:
        heights = jax.random.uniform(jax.random.fold_in(jax.random.fold_in(key, 6), dim), (blocks,), jnp.float32, smallest / len(cuts), top_value / len(cuts))
        level = level * jnp.repeat(jnp.exp(heights), extent[dim] // blocks).reshape((-1,) + (1,) * (len(extent) - 1 - dim))
    return level


def bell_draw(rng, shape, deviation, most, cuts=(), kind=jnp.bfloat16):
    values = jax.random.normal(rng, shape, jnp.float32) * deviation
    if len(cuts) > 0:
        values = levels(rng, shape, cuts, -0.22, 0.18) * values
    return jnp.clip(values, min=-most, max=most).astype(kind)


def setup_inputs(seed: int = 0) -> dict:
    splits = jax.random.split(jax.random.key(seed), 8)
    tokens = bell_draw(splits[0], (SEQS, SECTIONS, SPAN, D), 1.0, 6.0, ((0, 2), (1, 2), (2, 8)))
    ln_gain = jnp.clip(1.0 + 0.18 * jax.random.normal(splits[1], (D,), jnp.float32), 0.099609375, 1.8984375).astype(jnp.bfloat16)
    w_key = bell_draw(splits[2], (D, KVH * HD), D ** -0.5, 0.09375, ((0, 8),))
    w_value = bell_draw(splits[3], (D, KVH * HD), D ** -0.5, 0.09375, ((0, 8),))
    queries = bell_draw(splits[4], (PAIRS, GROUP * HD), 1.0, 6.0, ((0, 16),))
    head_shift = draw_head_shift(jax.random.fold_in(splits[7], 71), 0)
    key_shift = draw_key_shift(jax.random.fold_in(splits[7], 71), 0)
    return {"tokens": tokens, "ln_gain": ln_gain, "w_key": w_key, "w_value": w_value, "queries": queries, "head_shift": head_shift, "key_shift": key_shift}


epsilon = 1e-05

def project_sequence(block, ln_gain, w_key, w_value):
    flat_rows = block.reshape(LEN, D).astype(jnp.float32)
    row_mean = lax.optimization_barrier(jnp.mean(flat_rows, axis=1, keepdims=True))
    centred = flat_rows - row_mean
    row_var = lax.optimization_barrier(jnp.mean(centred * centred, axis=1, keepdims=True))
    normed = (centred * lax.rsqrt(row_var + epsilon) * ln_gain.astype(jnp.float32)).astype(jnp.bfloat16)
    keys = jnp.dot(normed, w_key, preferred_element_type=jnp.float32).astype(jnp.bfloat16)
    values = jnp.dot(normed, w_value, preferred_element_type=jnp.float32).astype(jnp.bfloat16)
    joined = jnp.concatenate([keys.reshape(LEN, KVH, HD), values.reshape(LEN, KVH, HD)], axis=2)
    return jnp.transpose(joined, (1, 0, 2))

def read_pair(pair_cache, query, shift_row, head_row):
    keys = pair_cache[:, :HD]
    values = pair_cache[:, HD:]
    logits = jnp.dot(query.reshape(GROUP, HD), keys.T, preferred_element_type=jnp.float32) * HD ** (-0.5)
    logits = logits + head_row[:, None] + shift_row[None, :]
    log_beta = jax.nn.log_sigmoid(logits)
    log_keep = (log_beta - logits).reshape(GROUP, SECTIONS, SPAN)
    within = lax.cumsum(log_keep, axis=2, reverse=True) - log_keep
    local_weight = jnp.exp(log_beta.reshape(GROUP, SECTIONS, SPAN) + within).astype(jnp.bfloat16)
    parts = jnp.einsum('gsj,sjd->gsd', local_weight.astype(jnp.float32), values.reshape(SECTIONS, SPAN, HD).astype(jnp.float32))
    totals = lax.optimization_barrier(jnp.sum(log_keep, axis=2))
    carry = lax.cumsum(totals, axis=1, reverse=True) - totals
    return lax.optimization_barrier(jnp.sum(jnp.exp(carry)[:, :, None] * parts, axis=1)).reshape(GROUP * HD)

def reference(tokens, ln_gain, w_key, w_value, queries, head_shift, key_shift):
    caches = lax.map(lambda block: project_sequence(block, ln_gain, w_key, w_value), tokens)
    kv_cache = caches.reshape(PAIRS, LEN, 2 * HD)
    head_rows = jnp.tile(head_shift, (SEQS, 1))
    first_read = lax.map(lambda items: read_pair(items[0], items[1], items[2], items[3]), (kv_cache, queries, key_shift, head_rows))
    return (kv_cache, first_read)
```

```python
import functools

import jax
import jax.numpy as jnp
from jax import lax
from jax.experimental import pallas as pl
from jax.experimental.pallas import tpu as pltpu
from jax.sharding import PartitionSpec as P

epsilon = 1e-05
LANES = 128
FILLS = 4
NORMS = 8
EARLY = 4
BASES = (0.0, 2.0, 4.0, 6.0)
LANE, GROUP_AT, PLACE_AT, CORNER_AT, TIMES_AT, OWN = 1.5, 3.0, 2.0, 5.0, 7.0, -1.0
NORM_START, NORM_STEP = 0.2, 0.6
CORNER = (("y", "x", "y", "x"), ("x", "y", "x", "y"))
MESH = pl.DeviceIdType.MESH


def layout(mesh):
    sp, gr, tp = mesh.shape["sp"], mesh.shape["gr"], mesh.shape["tp"]
    inner = 1
    while inner * inner * 4 <= sp and sp % (inner * 2) == 0:
        inner *= 2
    return sp // inner, inner, gr, tp


def nearest(depth):
    return [[lane] + sorted((k for k in range(depth) if k != lane), key=lambda k: (abs(k - lane), -k)) for lane in range(depth)]


def plan(blocks, depth):
    steps = []
    for i in range(NORMS):
        steps.append((NORM_START + i * NORM_STEP, "norm", i))
    for m in range(blocks):
        base = BASES[m % len(BASES)]
        steps.append((-50.0 + 0.01 * m if m < EARLY else base + OWN, "own", m))
        for r in range(depth):
            at = base + r * LANE
            if r:
                steps.append((at, "lane", m, r))
                steps.append((at + GROUP_AT, "group", m, r))
            steps.append((at + PLACE_AT, "place", m, r))
            steps.append((at + CORNER_AT, "corner", m, r))
            end = max(at + TIMES_AT, NORM_START + NORMS * NORM_STEP)
            steps.append((end, "times", m, r))
        steps.append((end + 0.001, "trade", m))
    return sorted(steps, key=lambda step: step[0])


def body(
    grid, head_size,
    tokens, gain_in, w_key, w_value, queries_in, head_shift_in, key_shift_in,
    cache, read,
    raw, normed, weights, acc, outgoing, incoming, totals, parts,
    gain, queries, head_shift, key_shift,
    send_sem, piece_sem, cross_sem, last_sem, load_sem,
):
    depth, inner, groups, sections = grid
    seats = depth * inner
    seat, group, section = lax.axis_index("sp"), lax.axis_index("gr"), lax.axis_index("tp")
    lane, place = seat // inner, seat % inner
    rows, width = raw.shape
    shard, columns = w_key.shape
    blocks, _, span = weights.shape
    piece = shard // (groups * sections)
    kv_heads, heads = head_shift.shape
    seqs = seats // kv_heads
    sub = rows // seqs
    half = sub // 2
    per_kind = columns // span
    per_block = span // head_size
    fill_rows = rows // FILLS
    norm_rows = rows // NORMS

    own = pl.ds(pl.multiple_of(seat * shard, shard), shard)
    loads = []
    for m in range(blocks):
        source = (w_key, w_value)[m // per_kind].at[:, pl.ds((m % per_kind) * span, span)]
        loads.append(pltpu.make_async_copy(source, weights.at[m, own], load_sem.at[m]))
        loads[-1].start()
    fills = []
    for at in range(FILLS):
        rows_at = pl.ds(at * fill_rows, fill_rows)
        fills.append(pltpu.make_async_copy(tokens.at[rows_at], raw.at[rows_at], load_sem.at[blocks + at]))
        fills[-1].start()
    smalls = []
    for at, (source, target) in enumerate(
        ((gain_in, gain), (queries_in, queries), (head_shift_in, head_shift), (key_shift_in, key_shift))
    ):
        smalls.append(pltpu.make_async_copy(source, target, load_sem.at[blocks + FILLS + at]))
        smalls[-1].start()

    barrier = pltpu.get_barrier_semaphore()

    def greet(**where):
        pl.semaphore_signal(barrier, 1, device_id=where, device_id_type=MESH)

    @pl.when(lane > 0)
    def _():
        greet(sp=seat - inner)

    @pl.when(lane < depth - 1)
    def _():
        greet(sp=seat + inner)

    for j in range(1, inner):
        greet(sp=lane * inner + lax.rem(place + j, inner))
    for g in range(1, groups):
        greet(gr=lax.rem(group + g, groups))
    for t in range(1, sections):
        greet(tp=lax.rem(section + t, sections))

    order = nearest(depth)

    def lane_at(r):
        found = order[depth - 1][r]
        for k in range(depth - 1):
            differs = (lax.rem(lane - k + depth, depth) + depth - 1) // depth
            found = found + (1 - differs) * (order[k][r] - order[depth - 1][r])
        return found

    ranks = [lane] + [lane_at(r) for r in range(1, depth)]

    def piece_at(m, r, j, g):
        at = ranks[r] * inner + lax.rem(place + j, inner)
        share = lax.rem(group + g, groups) * sections + section
        start = pl.multiple_of(at * shard + share * piece, piece)
        return weights.at[m, pl.ds(start, piece)], piece_sem.at[m, at, lax.rem(group + g, groups)]

    sent = [0] * blocks

    def push(source, target, out_sem, in_sem, **where):
        pltpu.make_async_remote_copy(
            src_ref=source, dst_ref=target, send_sem=out_sem, recv_sem=in_sem, device_id=where, device_id_type=MESH
        ).start()

    def settle(like, sem):
        pltpu.make_async_copy(like, like, sem).wait()

    def to_places(m, r, g):
        block, sem = piece_at(m, r, 0, g)
        for j in range(1, inner):
            push(block, block, send_sem.at[m], sem, sp=lane * inner + lax.rem(place + j, inner))
            sent[m] += 1

    def to_groups(m, r, j):
        block, sem = piece_at(m, r, j, 0)
        for g in range(1, groups):
            push(block, block, send_sem.at[m], sem, gr=lax.rem(group + g, groups))
            sent[m] += 1

    def to_sections(m, r, j, g):
        block, _ = piece_at(m, r, j, g)
        for t in range(1, sections):
            push(block, block, send_sem.at[m], cross_sem.at[m, r], tp=lax.rem(section + t, sections))
            sent[m] += 1

    def arrive(m, r, j, g):
        settle(*piece_at(m, r, j, g))

    def step_own(m):
        loads[m].wait()
        block, sem = piece_at(m, 0, 0, 0)

        @pl.when(lane > 0)
        def _():
            push(block, block, send_sem.at[blocks + m], sem, sp=seat - inner)

        @pl.when(lane < depth - 1)
        def _():
            push(block, block, send_sem.at[blocks + m], sem, sp=seat + inner)

        to_places(m, 0, 0)
        if CORNER[m % len(CORNER)][0] == "y":
            for g in range(1, groups):
                to_places(m, 0, g)

    def step_lane(m, r):
        arrive(m, r, 0, 0)
        block, sem = piece_at(m, r, 0, 0)
        above = (ranks[r] - lane + depth) // depth
        onward = lane + 1 - 2 * above

        @pl.when((onward >= 0) & (onward < depth))
        def _():
            push(block, block, send_sem.at[blocks + m], sem, sp=onward * inner + place)

        to_places(m, r, 0)
        to_groups(m, r, 0)
        to_sections(m, r, 0, 0)

    def corner(m, r):
        return CORNER[m % len(CORNER)][min(r, len(CORNER[0]) - 1)]

    def step_group(m, r):
        for g in range(1, groups):
            arrive(m, r, 0, g)
            if corner(m, r) == "y":
                to_places(m, r, g)
            to_sections(m, r, 0, g)

    def step_place(m, r):
        for j in range(1, inner):
            arrive(m, r, j, 0)
            if corner(m, r) == "x":
                to_groups(m, r, j)
            to_sections(m, r, j, 0)

    def step_corner(m, r):
        for j in range(1, inner):
            for g in range(1, groups):
                arrive(m, r, j, g)
                to_sections(m, r, j, g)

    def step_norm(i):
        if i == 0:
            smalls[0].wait()
        if i * norm_rows % fill_rows == 0:
            fills[i * norm_rows // fill_rows].wait()
        step = 32

        @pl.loop(0, norm_rows // step)
        def _(k):
            here = pl.ds(pl.multiple_of(i * norm_rows + k * step, step), step)
            x = raw[here, :].astype(jnp.float32)
            mean = jnp.mean(x, axis=1, keepdims=True)
            centred = x - mean
            var = jnp.mean(centred * centred, axis=1, keepdims=True)
            scale = gain[...].astype(jnp.float32).reshape(1, width)
            normed[here, :] = (centred * lax.rsqrt(var + epsilon) * scale).astype(jnp.bfloat16)

    def step_times(m, r):
        count = ((inner - 1) if r == 0 else inner) * groups * (sections - 1)
        if count:
            settle(weights.at[m, pl.ds(0, count * piece)], cross_sem.at[m, r])
        long = inner * shard
        start = pl.multiple_of(ranks[r] * long, long)
        out = jnp.dot(normed[:, pl.ds(start, long)], weights[m, pl.ds(start, long), :], preferred_element_type=jnp.float32)
        if r == 0:
            acc[m] = out
        else:
            acc[m] += out

    def step_trade(m):
        kind, part = m // per_kind, m % per_kind
        for seq in range(seqs):
            for i in range(per_block):
                cut = slice(i * head_size, (i + 1) * head_size)
                first = acc[m, seq * sub:seq * sub + half, cut]
                second = acc[m, seq * sub + half:(seq + 1) * sub, cut]
                outgoing[m, seq * per_block + i] = jnp.concatenate([first, second], axis=1).astype(jnp.bfloat16)
        home = seat // kv_heads
        for s in range(seqs):
            seq = lax.rem(home + 1 + s, seqs)
            for i in range(per_block):
                to = seq * kv_heads + part * per_block + i
                at = seq * per_block + i

                def send():
                    push(outgoing.at[m, at], incoming.at[kind, seat], last_sem.at[kind], last_sem.at[2 + kind], sp=to)

                if s < seqs - 1:
                    send()
                else:
                    pl.when(to != seat)(send)

                    @pl.when(to == seat)
                    def _():
                        incoming[kind, pl.ds(seat, 1)] = outgoing[m, pl.ds(at, 1)]

    pl.semaphore_wait(barrier, inner + groups + sections - 3 + (lane + depth - 1) // depth + (2 * depth - 2 - lane) // depth)
    calls = {
        "own": step_own, "lane": step_lane, "group": step_group, "place": step_place, "corner": step_corner,
        "norm": step_norm, "times": step_times, "trade": step_trade,
    }
    for _, name, *arguments in plan(blocks, depth):
        with jax.named_scope(name + "_" + "_".join(map(str, arguments))):
            calls[name](*arguments)

    for copy in smalls[1:]:
        copy.wait()
    query = queries[...].astype(jnp.float32)
    query = jnp.concatenate([query[:, g * head_size:(g + 1) * head_size] for g in range(heads)], axis=0)
    blank = jnp.zeros_like(query)
    query = jnp.concatenate(
        [jnp.concatenate([query, blank], axis=1), jnp.concatenate([blank, query], axis=1)], axis=0
    ).astype(jnp.bfloat16)
    mine = lax.broadcasted_iota(jnp.int32, (kv_heads, heads), 0) == lax.rem(seat, kv_heads)
    shift = jnp.sum(jnp.where(mine, head_shift[...], 0.0), axis=0, keepdims=True)
    eye = lax.broadcasted_iota(jnp.int32, (heads, heads), 0) == lax.broadcasted_iota(jnp.int32, (heads, heads), 1)
    shift = jnp.sum(jnp.where(eye, jnp.broadcast_to(shift, (heads, heads)), 0.0), axis=1, keepdims=True)
    later = (
        lax.broadcasted_iota(jnp.int32, (half, half), 0) > lax.broadcasted_iota(jnp.int32, (half, half), 1)
    ).astype(jnp.float32)

    with jax.named_scope("keys_in"):
        settle(incoming.at[0, pl.ds(0, seats - 1)], last_sem.at[2])
    trace = jax.named_scope("logits")
    trace.__enter__()
    keys = incoming[0].reshape(seats * half, 2 * head_size)
    logits = lax.dot_general(query, keys, (((1,), (1,)), ((), ())), preferred_element_type=jnp.float32)
    logits = logits * head_size ** (-0.5)
    betas, keeps = [], []
    for at in range(2 * seats):
        q, h = at // 2, at % 2
        z = logits[h * heads:(h + 1) * heads, q * half:(q + 1) * half]
        z = z + shift + key_shift[:, at * half:(at + 1) * half]
        tail = jnp.log1p(jnp.exp(-jnp.abs(z)))
        betas.append(jnp.minimum(z, 0.0) - tail)
        keeps.append(jnp.minimum(-z, 0.0) - tail)
    within = jnp.dot(
        jnp.concatenate(keeps, axis=0), later, preferred_element_type=jnp.float32, precision=lax.Precision.HIGHEST
    )
    running = jnp.zeros((heads, 1), jnp.float32)
    local = [None] * (2 * seats)
    for at in reversed(range(2 * seats)):
        local[at] = jnp.exp(betas[at] + within[at * heads:(at + 1) * heads] + running)
        running = running + jnp.sum(keeps[at], axis=1, keepdims=True)
    local = jnp.concatenate(
        [jnp.concatenate(local[0::2], axis=1), jnp.concatenate(local[1::2], axis=1)], axis=0
    ).astype(jnp.bfloat16)
    totals[section] = jnp.broadcast_to(running, totals.shape[1:])
    for t in range(1, sections):
        push(totals.at[section], totals.at[section], last_sem.at[4], last_sem.at[5], tp=lax.rem(section + t, sections))
    trace.__exit__(None, None, None)
    trace = jax.named_scope("totals_in")
    trace.__enter__()
    if sections > 1:
        settle(totals.at[pl.ds(0, sections - 1)], last_sem.at[5])
    carry = jnp.zeros((heads, head_size), jnp.float32)
    for t in reversed(range(sections)):
        carry = carry + jnp.where(section < t, totals[t][:, :head_size], 0.0)
    carry = jnp.exp(carry)
    trace.__exit__(None, None, None)

    with jax.named_scope("values_in"):
        settle(incoming.at[1, pl.ds(0, seats - 1)], last_sem.at[3])
    trace = jax.named_scope("part")
    trace.__enter__()
    values = incoming[1].reshape(seats * half, 2 * head_size)
    part = jnp.dot(local, values, preferred_element_type=jnp.float32)
    part = carry * (part[:heads, :head_size] + part[heads:, head_size:])
    parts[section] = jnp.concatenate([part, part], axis=1)
    for t in range(1, sections):
        push(parts.at[section], parts.at[section], last_sem.at[6], last_sem.at[7], tp=lax.rem(section + t, sections))
    trace.__exit__(None, None, None)
    trace = jax.named_scope("cache")
    trace.__enter__()
    for q in range(seats):
        for h in range(2):
            cut = slice(h * head_size, (h + 1) * head_size)
            start = (2 * q + h) * half
            cache[0, start:start + half, :] = jnp.concatenate([incoming[0, q][:, cut], incoming[1, q][:, cut]], axis=1)
    for m in range(blocks):
        settle(weights.at[m, pl.ds(0, sent[m] * piece)], send_sem.at[m])
        for k in range(depth):
            count = (k + 1 if k < depth - 1 else 0) + (depth - k if k > 0 else 0)
            if count:
                @pl.when(lane == k)
                def _():
                    settle(weights.at[m, pl.ds(0, count * piece)], send_sem.at[blocks + m])
    for kind in range(2):
        settle(incoming.at[kind, pl.ds(0, seats - 1)], last_sem.at[kind])
    trace.__exit__(None, None, None)
    trace = jax.named_scope("parts_in")
    trace.__enter__()
    if sections > 1:
        settle(totals.at[pl.ds(0, sections - 1)], last_sem.at[4])
        settle(parts.at[pl.ds(0, sections - 1)], last_sem.at[6])
        settle(parts.at[pl.ds(0, sections - 1)], last_sem.at[7])
    total = parts[0]
    for t in range(1, sections):
        total = total + parts[t]
    for g in range(heads):
        read[:, g * head_size:(g + 1) * head_size] = total[g:g + 1, :head_size]
    trace.__exit__(None, None, None)


def hand_over(cache, read, cache_out, read_out, sem):
    first = pltpu.make_async_copy(cache, cache_out, sem.at[0])
    second = pltpu.make_async_copy(read, read_out, sem.at[1])
    first.start()
    second.start()
    first.wait()
    second.wait()


def local(grid, tokens, ln_gain, w_key, w_value, queries, head_shift, key_shift):
    depth, inner, groups, sections = grid
    seats = depth * inner
    seqs, _, sub, width = tokens.shape
    rows = seqs * sub
    columns = w_key.shape[1]
    kv_heads, heads = head_shift.shape
    head_size = columns // kv_heads
    blocks = 2 * columns // LANES
    vmem = pl.BlockSpec(memory_space=pltpu.VMEM)
    hbm = pl.BlockSpec(memory_space=pl.ANY)
    operands = (tokens.reshape(rows, width), ln_gain, w_key, w_value, queries, head_shift, key_shift)
    cache, read = pl.pallas_call(
        functools.partial(body, grid, head_size),
        out_shape=(
            jax.ShapeDtypeStruct((1, seats * sub, 2 * head_size), jnp.bfloat16),
            jax.ShapeDtypeStruct((1, heads * head_size), jnp.float32),
        ),
        in_specs=[hbm] * len(operands),
        out_specs=(vmem, vmem),
        scratch_shapes=[
            pltpu.VMEM((rows, width), jnp.bfloat16),
            pltpu.VMEM((rows, width), jnp.bfloat16),
            pltpu.VMEM((blocks, width, LANES), jnp.bfloat16),
            pltpu.VMEM((blocks, rows, LANES), jnp.float32),
            pltpu.VMEM((blocks, seqs * LANES // head_size, sub // 2, 2 * head_size), jnp.bfloat16),
            pltpu.VMEM((2, seats, sub // 2, 2 * head_size), jnp.bfloat16),
            pltpu.VMEM((sections, heads, 2 * head_size), jnp.float32),
            pltpu.VMEM((sections, heads, 2 * head_size), jnp.float32),
            pltpu.VMEM(ln_gain.shape, ln_gain.dtype),
            pltpu.VMEM(queries.shape, queries.dtype),
            pltpu.VMEM(head_shift.shape, head_shift.dtype),
            pltpu.VMEM(key_shift.shape, key_shift.dtype),
            pltpu.SemaphoreType.DMA((2 * blocks,)),
            pltpu.SemaphoreType.DMA((blocks, seats, groups)),
            pltpu.SemaphoreType.DMA((blocks, depth)),
            pltpu.SemaphoreType.DMA((8,)),
            pltpu.SemaphoreType.DMA((blocks + FILLS + 4,)),
        ],
        compiler_params=pltpu.CompilerParams(
            collective_id=0, has_side_effects=True, vmem_limit_bytes=24 * 1024 * 1024
        ),
    )(*(pltpu.with_memory_space_constraint(x, pltpu.HBM) for x in operands))
    return pl.pallas_call(
        hand_over,
        out_shape=(jax.ShapeDtypeStruct(cache.shape, cache.dtype), jax.ShapeDtypeStruct(read.shape, read.dtype)),
        in_specs=[vmem, vmem],
        out_specs=(hbm, hbm),
        scratch_shapes=[pltpu.SemaphoreType.DMA((2,))],
        compiler_params=pltpu.CompilerParams(vmem_limit_bytes=4 * 1024 * 1024),
    )(cache, read)


def solution(mesh):
    in_specs = (
        P("gr", "tp", "sp", None),
        P(),
        P("sp", None),
        P("sp", None),
        P(("gr", "sp"), None),
        P(),
        P(("gr", "sp"), "tp"),
    )
    out_specs = (P(("gr", "sp"), "tp", None), P(("gr", "sp"), None))
    return jax.shard_map(
        functools.partial(local, layout(mesh)), mesh=mesh, in_specs=in_specs, out_specs=out_specs, check_vma=False
    )
```

```python
import functools

import jax
import jax.numpy as jnp
from jax import lax
from jax.experimental import pallas as pl
from jax.experimental.pallas import tpu as pltpu
from jax.sharding import PartitionSpec as P

epsilon = 1e-05
LANES = 128
NORM, OWN, HOP, GROUP, PLACE, EDGE, TIMES, PAIR, TRADE = range(9)
FILLS = 4
NORMS = 8
BASES = (0.0, 2.0, 4.0, 6.0)
LANE_STEP, GROUP_AT, PLACE_AT, CORNER_AT, TIMES_AT, OWN_AT = 1.5, 3.0, 2.0, 5.0, 7.0, -3.0
NORM_START, NORM_STEP = 0.2, 0.6
CORNER = (("y", "y", "y", "y"), ("x", "x", "y", "x"), ("x", "x", "y", "x"), ("x", "x", "x", "x"))
ORDER = (
    (OWN, 0, 0), (NORM, 4, 0), (OWN, 1, 0), (OWN, 2, 0), (OWN, 3, 0), (NORM, 7, 0),
    (NORM, 5, 0), (NORM, 2, 0), (HOP, 0, 2), (HOP, 0, 1), (HOP, 1, 2), (HOP, 1, 1),
    (PLACE, 2, 0), (PLACE, 0, 0), (GROUP, 0, 1), (HOP, 0, 3), (GROUP, 0, 2), (HOP, 1, 3),
    (HOP, 2, 1), (NORM, 6, 0), (NORM, 1, 0), (PLACE, 1, 1), (PLACE, 0, 1), (PLACE, 0, 2),
    (GROUP, 0, 3), (HOP, 2, 2), (GROUP, 1, 2), (NORM, 3, 0), (PLACE, 1, 0), (GROUP, 1, 1),
    (NORM, 0, 0), (HOP, 2, 3), (EDGE, 0, 0), (PLACE, 1, 3), (EDGE, 0, 1), (PLACE, 0, 3),
    (EDGE, 0, 2), (PLACE, 2, 1), (HOP, 3, 1), (EDGE, 0, 3), (HOP, 3, 2), (GROUP, 2, 2),
    (GROUP, 1, 3), (TIMES, 0, 0), (EDGE, 1, 0), (GROUP, 2, 1), (EDGE, 1, 1), (PLACE, 1, 2),
    (EDGE, 2, 0), (EDGE, 1, 2), (PLACE, 2, 3), (TIMES, 0, 1), (TIMES, 0, 3), (EDGE, 1, 3),
    (HOP, 3, 3), (TIMES, 0, 2), (TRADE, 0, 0), (GROUP, 3, 1), (PLACE, 2, 2), (TIMES, 1, 0),
    (PLACE, 3, 1), (PLACE, 3, 2), (EDGE, 2, 1), (TIMES, 1, 1), (EDGE, 2, 2), (GROUP, 2, 3),
    (TIMES, 1, 2), (TIMES, 1, 3), (PLACE, 3, 0), (EDGE, 2, 3), (TRADE, 1, 0), (TIMES, 2, 1),
    (PLACE, 3, 3), (TIMES, 2, 2), (GROUP, 3, 2), (TIMES, 2, 0), (EDGE, 3, 0), (TIMES, 2, 3),
    (TRADE, 2, 0), (EDGE, 3, 1), (EDGE, 3, 3), (GROUP, 3, 3), (EDGE, 3, 2), (TIMES, 3, 2),
    (TIMES, 3, 3), (TIMES, 3, 1), (TIMES, 3, 0), (TRADE, 3, 0),
)
MESH = pl.DeviceIdType.MESH


def layout(mesh):
    sp, gr, tp = mesh.shape["sp"], mesh.shape["gr"], mesh.shape["tp"]
    inner = 1
    while inner * inner * 4 <= sp and sp % (inner * 2) == 0:
        inner *= 2
    return sp // inner, inner, gr, tp


def nearest(depth):
    return [[lane] + sorted((k for k in range(depth) if k != lane), key=lambda k: (abs(k - lane), -k)) for lane in range(depth)]


def plan(blocks, depth):
    if (blocks, depth) == (len(CORNER), len(CORNER[0])):
        return ORDER
    steps = []
    for i in range(NORMS):
        steps.append((NORM_START + i * NORM_STEP, NORM, i, 0))
    for m in range(blocks):
        base = BASES[m % len(BASES)]
        steps.append((base + OWN_AT, OWN, m, 0))
        for r in range(depth):
            at = base + r * LANE_STEP
            if r:
                steps.append((at, HOP, m, r))
                steps.append((at + GROUP_AT, GROUP, m, r))
            steps.append((at + PLACE_AT, PLACE, m, r))
            steps.append((at + CORNER_AT, EDGE, m, r))
            end = max(at + TIMES_AT, NORM_START + NORMS * NORM_STEP)
            steps.append((end, TIMES, m, r))
        steps.append((end + 0.001, TRADE, m, 0))
    return [step[1:] for step in sorted(steps, key=lambda step: step[0])]


def body(
    grid, head_size,
    tokens, gain_in, w_key, w_value, queries_in, head_shift_in, key_shift_in,
    cache, read,
    raw, normed, weights, acc, outgoing, incoming, totals, parts,
    gain, queries, head_shift, key_shift,
    send_sem, piece_sem, cross_sem, last_sem, load_sem,
):
    depth, inner, groups, sections = grid
    seats = depth * inner
    seat, group, section = lax.axis_index("sp"), lax.axis_index("gr"), lax.axis_index("tp")
    lane, place = seat // inner, seat % inner
    rows, width = raw.shape
    shard, columns = w_key.shape
    blocks, _, span = weights.shape
    piece = shard // (groups * sections)
    kv_heads, heads = head_shift.shape
    seqs = seats // kv_heads
    sub = rows // seqs
    half = sub // 2
    per_kind = columns // span
    per_block = span // head_size
    fill_rows = rows // FILLS
    norm_rows = rows // NORMS

    own = pl.ds(pl.multiple_of(seat * shard, shard), shard)
    loads = []
    for m in range(blocks):
        source = (w_key, w_value)[m // per_kind].at[:, pl.ds((m % per_kind) * span, span)]
        loads.append(pltpu.make_async_copy(source, weights.at[m, own], load_sem.at[m]))
        loads[-1].start()
    fills = []
    for at in range(FILLS):
        rows_at = pl.ds(at * fill_rows, fill_rows)
        fills.append(pltpu.make_async_copy(tokens.at[rows_at], raw.at[rows_at], load_sem.at[blocks + at]))
        fills[-1].start()
    smalls = []
    for at, (source, target) in enumerate(
        ((gain_in, gain), (queries_in, queries), (head_shift_in, head_shift), (key_shift_in, key_shift))
    ):
        smalls.append(pltpu.make_async_copy(source, target, load_sem.at[blocks + FILLS + at]))
        smalls[-1].start()

    barrier = pltpu.get_barrier_semaphore()

    def greet(**where):
        pl.semaphore_signal(barrier, 1, device_id=where, device_id_type=MESH)

    @pl.when(lane > 0)
    def _():
        greet(sp=seat - inner)

    @pl.when(lane < depth - 1)
    def _():
        greet(sp=seat + inner)

    for j in range(1, inner):
        greet(sp=lane * inner + lax.rem(place + j, inner))
    for g in range(1, groups):
        greet(gr=lax.rem(group + g, groups))
    for t in range(1, sections):
        greet(tp=lax.rem(section + t, sections))

    order = nearest(depth)

    def lane_at(r):
        found = order[depth - 1][r]
        for k in range(depth - 1):
            differs = (lax.rem(lane - k + depth, depth) + depth - 1) // depth
            found = found + (1 - differs) * (order[k][r] - order[depth - 1][r])
        return found

    ranks = [lane] + [lane_at(r) for r in range(1, depth)]

    def piece_at(m, r, j, g):
        at = ranks[r] * inner + lax.rem(place + j, inner)
        share = lax.rem(group + g, groups) * sections + section
        start = pl.multiple_of(at * shard + share * piece, piece)
        return weights.at[m, pl.ds(start, piece)], piece_sem.at[m, at, lax.rem(group + g, groups)]

    sent = [0] * blocks

    def push(source, target, out_sem, in_sem, **where):
        pltpu.make_async_remote_copy(
            src_ref=source, dst_ref=target, send_sem=out_sem, recv_sem=in_sem, device_id=where, device_id_type=MESH
        ).start()

    def settle(like, sem):
        pltpu.make_async_copy(like, like, sem).wait()

    def to_places(m, r, g):
        block, sem = piece_at(m, r, 0, g)
        for j in range(1, inner):
            push(block, block, send_sem.at[m], sem, sp=lane * inner + lax.rem(place + j, inner))
            sent[m] += 1

    def to_groups(m, r, j):
        block, sem = piece_at(m, r, j, 0)
        for g in range(1, groups):
            push(block, block, send_sem.at[m], sem, gr=lax.rem(group + g, groups))
            sent[m] += 1

    def to_sections(m, r, j, g):
        block, _ = piece_at(m, r, j, g)
        for t in range(1, sections):
            push(block, block, send_sem.at[m], cross_sem.at[m, r], tp=lax.rem(section + t, sections))
            sent[m] += 1

    def arrive(m, r, j, g):
        settle(*piece_at(m, r, j, g))

    def step_own(m, _):
        loads[m].wait()
        block, sem = piece_at(m, 0, 0, 0)

        @pl.when(lane > 0)
        def _():
            push(block, block, send_sem.at[blocks + m], sem, sp=seat - inner)

        @pl.when(lane < depth - 1)
        def _():
            push(block, block, send_sem.at[blocks + m], sem, sp=seat + inner)

        to_places(m, 0, 0)
        if CORNER[m % len(CORNER)][0] == "y":
            for g in range(1, groups):
                to_places(m, 0, g)

    def step_lane(m, r):
        arrive(m, r, 0, 0)
        block, sem = piece_at(m, r, 0, 0)
        above = (ranks[r] - lane + depth) // depth
        onward = lane + 1 - 2 * above

        @pl.when((onward >= 0) & (onward < depth))
        def _():
            push(block, block, send_sem.at[blocks + m], sem, sp=onward * inner + place)

        to_places(m, r, 0)
        to_groups(m, r, 0)
        to_sections(m, r, 0, 0)

    def corner(m, r):
        return CORNER[m % len(CORNER)][min(r, len(CORNER[0]) - 1)]

    def step_group(m, r):
        for g in range(1, groups):
            arrive(m, r, 0, g)
            if corner(m, r) == "y":
                to_places(m, r, g)
            to_sections(m, r, 0, g)

    def step_place(m, r):
        for j in range(1, inner):
            arrive(m, r, j, 0)
            if corner(m, r) == "x":
                to_groups(m, r, j)
            to_sections(m, r, j, 0)

    def step_corner(m, r):
        for j in range(1, inner):
            for g in range(1, groups):
                arrive(m, r, j, g)
                to_sections(m, r, j, g)

    filled, begun = set(), set()

    def add(m, out):
        if m in begun:
            acc[m] += out
        else:
            acc[m] = out
            begun.add(m)

    def step_norm(i, _):
        if not filled:
            smalls[0].wait()
        stage = i * norm_rows // fill_rows
        if stage not in filled:
            fills[stage].wait()
            filled.add(stage)
        step = 32

        @pl.loop(0, norm_rows // step)
        def _(k):
            here = pl.ds(pl.multiple_of(i * norm_rows + k * step, step), step)
            x = raw[here, :].astype(jnp.float32)
            mean = jnp.mean(x, axis=1, keepdims=True)
            centred = x - mean
            var = jnp.mean(centred * centred, axis=1, keepdims=True)
            scale = gain[...].astype(jnp.float32).reshape(1, width)
            normed[here, :] = (centred * lax.rsqrt(var + epsilon) * scale).astype(jnp.bfloat16)

    def crossed(m, r):
        count = ((inner - 1) if r == 0 else inner) * groups * (sections - 1)
        if count:
            settle(weights.at[m, pl.ds(0, count * piece)], cross_sem.at[m, r])

    def step_pair(k, r):
        crossed(2 * k, r)
        crossed(2 * k + 1, r)
        long = inner * shard
        start = pl.multiple_of(ranks[r] * long, long)
        both = jnp.concatenate([weights[2 * k, pl.ds(start, long), :], weights[2 * k + 1, pl.ds(start, long), :]], axis=1)
        out = jnp.dot(normed[:, pl.ds(start, long)], both, preferred_element_type=jnp.float32)
        for m in range(2):
            add(2 * k + m, out[:, m * span:(m + 1) * span])

    def step_times(m, r):
        crossed(m, r)
        long = inner * shard
        start = pl.multiple_of(ranks[r] * long, long)
        out = jnp.dot(normed[:, pl.ds(start, long)], weights[m, pl.ds(start, long), :], preferred_element_type=jnp.float32)
        add(m, out)

    def step_trade(m, _):
        kind, part = m // per_kind, m % per_kind
        for seq in range(seqs):
            for i in range(per_block):
                cut = slice(i * head_size, (i + 1) * head_size)
                first = acc[m, seq * sub:seq * sub + half, cut]
                second = acc[m, seq * sub + half:(seq + 1) * sub, cut]
                outgoing[m, seq * per_block + i] = jnp.concatenate([first, second], axis=1).astype(jnp.bfloat16)
        home = seat // kv_heads
        for s in range(seqs):
            seq = lax.rem(home + 1 + s, seqs)
            for i in range(per_block):
                to = seq * kv_heads + part * per_block + i
                at = seq * per_block + i

                def send():
                    push(outgoing.at[m, at], incoming.at[kind, seat], last_sem.at[kind], last_sem.at[2 + kind], sp=to)

                if s < seqs - 1:
                    send()
                else:
                    pl.when(to != seat)(send)

                    @pl.when(to == seat)
                    def _():
                        incoming[kind, pl.ds(seat, 1)] = outgoing[m, pl.ds(at, 1)]

    pl.semaphore_wait(barrier, inner + groups + sections - 3 + (lane + depth - 1) // depth + (2 * depth - 2 - lane) // depth)
    calls = (step_norm, step_own, step_lane, step_group, step_place, step_corner, step_times, step_pair, step_trade)
    for which, m, r in plan(blocks, depth):
        with jax.named_scope(f"{calls[which].__name__}_{m}_{r}"):
            calls[which](m, r)

    for copy in smalls[1:]:
        copy.wait()
    query = queries[...].astype(jnp.float32)
    query = jnp.concatenate([query[:, g * head_size:(g + 1) * head_size] for g in range(heads)], axis=0)
    blank = jnp.zeros_like(query)
    query = jnp.concatenate(
        [jnp.concatenate([query, blank], axis=1), jnp.concatenate([blank, query], axis=1)], axis=0
    ).astype(jnp.bfloat16)
    mine = lax.broadcasted_iota(jnp.int32, (kv_heads, heads), 0) == lax.rem(seat, kv_heads)
    shift = jnp.sum(jnp.where(mine, head_shift[...], 0.0), axis=0, keepdims=True)
    eye = lax.broadcasted_iota(jnp.int32, (heads, heads), 0) == lax.broadcasted_iota(jnp.int32, (heads, heads), 1)
    shift = jnp.sum(jnp.where(eye, jnp.broadcast_to(shift, (heads, heads)), 0.0), axis=1, keepdims=True)
    later = (
        lax.broadcasted_iota(jnp.int32, (half, half), 0) > lax.broadcasted_iota(jnp.int32, (half, half), 1)
    ).astype(jnp.float32)

    with jax.named_scope("keys_in"):
        settle(incoming.at[0, pl.ds(0, seats - 1)], last_sem.at[2])
    trace = jax.named_scope("logits")
    trace.__enter__()
    keys = incoming[0].reshape(seats * half, 2 * head_size)
    logits = lax.dot_general(query, keys, (((1,), (1,)), ((), ())), preferred_element_type=jnp.float32)
    logits = logits * head_size ** (-0.5)
    betas, keeps = [], []
    for at in range(2 * seats):
        q, h = at // 2, at % 2
        z = logits[h * heads:(h + 1) * heads, q * half:(q + 1) * half]
        z = z + shift + key_shift[:, at * half:(at + 1) * half]
        tail = jnp.log1p(jnp.exp(-jnp.abs(z)))
        betas.append(jnp.minimum(z, 0.0) - tail)
        keeps.append(jnp.minimum(-z, 0.0) - tail)
    within = jnp.dot(
        jnp.concatenate(keeps, axis=0), later, preferred_element_type=jnp.float32, precision=lax.Precision.HIGHEST
    )
    running = jnp.zeros((heads, 1), jnp.float32)
    local = [None] * (2 * seats)
    for at in reversed(range(2 * seats)):
        local[at] = jnp.exp(betas[at] + within[at * heads:(at + 1) * heads] + running)
        running = running + jnp.sum(keeps[at], axis=1, keepdims=True)
    local = jnp.concatenate(
        [jnp.concatenate(local[0::2], axis=1), jnp.concatenate(local[1::2], axis=1)], axis=0
    ).astype(jnp.bfloat16)
    totals[section] = jnp.broadcast_to(running, totals.shape[1:])
    for t in range(1, sections):
        push(totals.at[section], totals.at[section], last_sem.at[4], last_sem.at[5], tp=lax.rem(section + t, sections))
    trace.__exit__(None, None, None)
    trace = jax.named_scope("totals_in")
    trace.__enter__()
    if sections > 1:
        settle(totals.at[pl.ds(0, sections - 1)], last_sem.at[5])
    carry = jnp.zeros((heads, head_size), jnp.float32)
    for t in reversed(range(sections)):
        carry = carry + jnp.where(section < t, totals[t][:, :head_size], 0.0)
    carry = jnp.exp(carry)
    trace.__exit__(None, None, None)

    with jax.named_scope("values_in"):
        settle(incoming.at[1, pl.ds(0, seats - 1)], last_sem.at[3])
    trace = jax.named_scope("part")
    trace.__enter__()
    values = incoming[1].reshape(seats * half, 2 * head_size)
    part = jnp.dot(local, values, preferred_element_type=jnp.float32)
    part = carry * (part[:heads, :head_size] + part[heads:, head_size:])
    parts[section] = jnp.concatenate([part, part], axis=1)
    for t in range(1, sections):
        push(parts.at[section], parts.at[section], last_sem.at[6], last_sem.at[7], tp=lax.rem(section + t, sections))
    trace.__exit__(None, None, None)
    trace = jax.named_scope("cache")
    trace.__enter__()
    for q in range(seats):
        for h in range(2):
            cut = slice(h * head_size, (h + 1) * head_size)
            start = (2 * q + h) * half
            cache[0, start:start + half, :] = jnp.concatenate([incoming[0, q][:, cut], incoming[1, q][:, cut]], axis=1)
    for m in range(blocks):
        settle(weights.at[m, pl.ds(0, sent[m] * piece)], send_sem.at[m])
        for k in range(depth):
            count = (k + 1 if k < depth - 1 else 0) + (depth - k if k > 0 else 0)
            if count:
                @pl.when(lane == k)
                def _():
                    settle(weights.at[m, pl.ds(0, count * piece)], send_sem.at[blocks + m])
    for kind in range(2):
        settle(incoming.at[kind, pl.ds(0, seats - 1)], last_sem.at[kind])
    trace.__exit__(None, None, None)
    trace = jax.named_scope("parts_in")
    trace.__enter__()
    if sections > 1:
        settle(totals.at[pl.ds(0, sections - 1)], last_sem.at[4])
        settle(parts.at[pl.ds(0, sections - 1)], last_sem.at[6])
        settle(parts.at[pl.ds(0, sections - 1)], last_sem.at[7])
    total = parts[0]
    for t in range(1, sections):
        total = total + parts[t]
    for g in range(heads):
        read[:, g * head_size:(g + 1) * head_size] = total[g:g + 1, :head_size]
    trace.__exit__(None, None, None)


def hand_over(cache, read, cache_out, read_out, sem):
    first = pltpu.make_async_copy(cache, cache_out, sem.at[0])
    second = pltpu.make_async_copy(read, read_out, sem.at[1])
    first.start()
    second.start()
    first.wait()
    second.wait()


def local(grid, tokens, ln_gain, w_key, w_value, queries, head_shift, key_shift):
    depth, inner, groups, sections = grid
    seats = depth * inner
    seqs, _, sub, width = tokens.shape
    rows = seqs * sub
    columns = w_key.shape[1]
    kv_heads, heads = head_shift.shape
    head_size = columns // kv_heads
    blocks = 2 * columns // LANES
    vmem = pl.BlockSpec(memory_space=pltpu.VMEM)
    hbm = pl.BlockSpec(memory_space=pl.ANY)
    operands = (tokens.reshape(rows, width), ln_gain, w_key, w_value, queries, head_shift, key_shift)
    cache, read = pl.pallas_call(
        functools.partial(body, grid, head_size),
        out_shape=(
            jax.ShapeDtypeStruct((1, seats * sub, 2 * head_size), jnp.bfloat16),
            jax.ShapeDtypeStruct((1, heads * head_size), jnp.float32),
        ),
        in_specs=[hbm] * len(operands),
        out_specs=(vmem, vmem),
        scratch_shapes=[
            pltpu.VMEM((rows, width), jnp.bfloat16),
            pltpu.VMEM((rows, width), jnp.bfloat16),
            pltpu.VMEM((blocks, width, LANES), jnp.bfloat16),
            pltpu.VMEM((blocks, rows, LANES), jnp.float32),
            pltpu.VMEM((blocks, seqs * LANES // head_size, sub // 2, 2 * head_size), jnp.bfloat16),
            pltpu.VMEM((2, seats, sub // 2, 2 * head_size), jnp.bfloat16),
            pltpu.VMEM((sections, heads, 2 * head_size), jnp.float32),
            pltpu.VMEM((sections, heads, 2 * head_size), jnp.float32),
            pltpu.VMEM(ln_gain.shape, ln_gain.dtype),
            pltpu.VMEM(queries.shape, queries.dtype),
            pltpu.VMEM(head_shift.shape, head_shift.dtype),
            pltpu.VMEM(key_shift.shape, key_shift.dtype),
            pltpu.SemaphoreType.DMA((2 * blocks,)),
            pltpu.SemaphoreType.DMA((blocks, seats, groups)),
            pltpu.SemaphoreType.DMA((blocks, depth)),
            pltpu.SemaphoreType.DMA((8,)),
            pltpu.SemaphoreType.DMA((blocks + FILLS + 4,)),
        ],
        compiler_params=pltpu.CompilerParams(
            collective_id=0, has_side_effects=True, vmem_limit_bytes=24 * 1024 * 1024
        ),
    )(*(pltpu.with_memory_space_constraint(x, pltpu.HBM) for x in operands))
    return pl.pallas_call(
        hand_over,
        out_shape=(jax.ShapeDtypeStruct(cache.shape, cache.dtype), jax.ShapeDtypeStruct(read.shape, read.dtype)),
        in_specs=[vmem, vmem],
        out_specs=(hbm, hbm),
        scratch_shapes=[pltpu.SemaphoreType.DMA((2,))],
        compiler_params=pltpu.CompilerParams(vmem_limit_bytes=4 * 1024 * 1024),
    )(cache, read)


def solution(mesh):
    in_specs = (
        P("gr", "tp", "sp", None),
        P(),
        P("sp", None),
        P("sp", None),
        P(("gr", "sp"), None),
        P(),
        P(("gr", "sp"), "tp"),
    )
    out_specs = (P(("gr", "sp"), "tp", None), P(("gr", "sp"), None))
    return jax.shard_map(
        functools.partial(local, layout(mesh)), mesh=mesh, in_specs=in_specs, out_specs=out_specs, check_vma=False
    )
```

```python
import functools

import jax
import jax.numpy as jnp
from jax import lax
from jax.experimental import pallas as pl
from jax.experimental.pallas import tpu as pltpu
from jax.sharding import PartitionSpec as P

epsilon = 1e-05
LANES = 128
NORM, OWN, HOP, GROUP, PLACE, EDGE, TIMES, PAIR, TRADE = range(9)
FILLS = 4
NORMS = 8
BASES = (0.0, 2.0, 4.0, 6.0)
LANE_STEP, GROUP_AT, PLACE_AT, CORNER_AT, TIMES_AT, OWN_AT = 1.5, 3.0, 2.0, 5.0, 7.0, -3.0
NORM_START, NORM_STEP = 0.2, 0.6
CORNER = (("y", "x", "x", "x"), ("y", "y", "x", "x"), ("x", "y", "y", "x"), ("x", "x", "y", "x"))
OUTER = (False, False, True, True)
ORDER = (
    (OWN, 0, 0), (OWN, 1, 0), (NORM, 7, 0), (OWN, 3, 0), (OWN, 2, 0), (NORM, 2, 0),
    (HOP, 0, 1), (NORM, 5, 0), (HOP, 1, 1), (HOP, 0, 2), (EDGE, 1, 0), (HOP, 0, 3),
    (HOP, 1, 2), (NORM, 0, 0), (HOP, 1, 3), (GROUP, 3, 1), (NORM, 4, 0), (HOP, 2, 1),
    (GROUP, 1, 1), (GROUP, 0, 1), (PLACE, 0, 2), (PLACE, 0, 1), (NORM, 3, 0), (EDGE, 0, 0),
    (GROUP, 0, 2), (HOP, 3, 1), (HOP, 2, 2), (PLACE, 1, 1), (PLACE, 0, 3), (NORM, 6, 0),
    (HOP, 2, 3), (PLACE, 2, 0), (PLACE, 1, 2), (NORM, 1, 0), (PLACE, 1, 3), (PLACE, 1, 0),
    (TIMES, 1, 0), (PLACE, 3, 0), (EDGE, 0, 2), (TIMES, 0, 2), (EDGE, 0, 1), (GROUP, 1, 3),
    (GROUP, 2, 1), (TIMES, 0, 1), (HOP, 3, 2), (GROUP, 0, 3), (PLACE, 0, 0), (TIMES, 0, 0),
    (GROUP, 2, 2), (EDGE, 1, 1), (HOP, 3, 3), (PLACE, 2, 1), (EDGE, 0, 3), (TIMES, 0, 3),
    (TRADE, 0, 0), (EDGE, 1, 2), (EDGE, 2, 1), (TIMES, 1, 1), (GROUP, 2, 3), (EDGE, 1, 3),
    (EDGE, 2, 0), (GROUP, 1, 2), (PLACE, 2, 3), (PLACE, 3, 2), (PLACE, 3, 1), (TIMES, 1, 3),
    (EDGE, 2, 2), (EDGE, 3, 0), (PLACE, 2, 2), (TIMES, 1, 2), (TRADE, 1, 0), (TIMES, 3, 0),
    (GROUP, 3, 2), (TIMES, 2, 1), (PLACE, 3, 3), (TIMES, 2, 2), (GROUP, 3, 3), (EDGE, 2, 3),
    (TIMES, 2, 0), (TIMES, 2, 3), (TRADE, 2, 0), (EDGE, 3, 1), (TIMES, 3, 1), (EDGE, 3, 3),
    (TIMES, 3, 3), (EDGE, 3, 2), (TIMES, 3, 2), (TRADE, 3, 0),
)
MESH = pl.DeviceIdType.MESH


def layout(mesh):
    sp, gr, tp = mesh.shape["sp"], mesh.shape["gr"], mesh.shape["tp"]
    inner = 1
    while inner * inner * 4 <= sp and sp % (inner * 2) == 0:
        inner *= 2
    return sp // inner, inner, gr, tp


def nearest(depth):
    return [[lane] + sorted((k for k in range(depth) if k != lane), key=lambda k: (abs(k - lane), k if 2 * lane < depth else -k)) for lane in range(depth)]


def plan(blocks, depth):
    if (blocks, depth) == (len(CORNER), len(CORNER[0])):
        return ORDER
    steps = []
    for i in range(NORMS):
        steps.append((NORM_START + i * NORM_STEP, NORM, i, 0))
    for m in range(blocks):
        base = BASES[m % len(BASES)]
        steps.append((base + OWN_AT, OWN, m, 0))
        for r in range(depth):
            at = base + r * LANE_STEP
            if r:
                steps.append((at, HOP, m, r))
                steps.append((at + GROUP_AT, GROUP, m, r))
            steps.append((at + PLACE_AT, PLACE, m, r))
            steps.append((at + CORNER_AT, EDGE, m, r))
            end = max(at + TIMES_AT, NORM_START + NORMS * NORM_STEP)
            steps.append((end, TIMES, m, r))
        steps.append((end + 0.001, TRADE, m, 0))
    return [step[1:] for step in sorted(steps, key=lambda step: step[0])]


def body(
    grid, head_size,
    tokens, gain_in, w_key, w_value, queries_in, head_shift_in, key_shift_in,
    cache, read,
    raw, normed, weights, acc, outgoing, incoming, totals, parts,
    gain, queries, head_shift, key_shift,
    send_sem, piece_sem, cross_sem, last_sem, load_sem,
):
    depth, inner, groups, sections = grid
    seats = depth * inner
    seat, group, section = lax.axis_index("sp"), lax.axis_index("gr"), lax.axis_index("tp")
    lane, place = seat // inner, seat % inner
    rows, width = raw.shape
    shard, columns = w_key.shape
    blocks, _, span = weights.shape
    leads = sections if sections > 2 else 1
    leading = section == sections - 1
    piece = shard // (groups * leads)
    kv_heads, heads = head_shift.shape
    seqs = seats // kv_heads
    sub = rows // seqs
    half = sub // 2
    per_kind = columns // span
    per_block = span // head_size
    fill_rows = rows // FILLS
    norm_rows = rows // NORMS

    own = pl.ds(pl.multiple_of(seat * shard, shard), shard)
    loads = []
    for m in range(blocks):
        source = (w_key, w_value)[m // per_kind].at[:, pl.ds((m % per_kind) * span, span)]
        loads.append(pltpu.make_async_copy(source, weights.at[m, own], load_sem.at[m]))
        loads[-1].start()
    fills = []
    for at in range(FILLS):
        rows_at = pl.ds(at * fill_rows, fill_rows)
        fills.append(pltpu.make_async_copy(tokens.at[rows_at], raw.at[rows_at], load_sem.at[blocks + at]))
        fills[-1].start()
    smalls = []
    for at, (source, target) in enumerate(
        ((gain_in, gain), (queries_in, queries), (head_shift_in, head_shift), (key_shift_in, key_shift))
    ):
        smalls.append(pltpu.make_async_copy(source, target, load_sem.at[blocks + FILLS + at]))
        smalls[-1].start()

    barrier = pltpu.get_barrier_semaphore()

    def greet(**where):
        pl.semaphore_signal(barrier, 1, device_id=where, device_id_type=MESH)

    @pl.when(lane > 0)
    def _():
        greet(sp=seat - inner)

    @pl.when(lane < depth - 1)
    def _():
        greet(sp=seat + inner)

    for j in range(1, inner):
        greet(sp=lane * inner + lax.rem(place + j, inner))
    for g in range(1, groups):
        greet(gr=lax.rem(group + g, groups))
    for t in range(1, sections):
        greet(tp=lax.rem(section + t, sections))

    order = nearest(depth)

    def lane_at(r):
        found = order[depth - 1][r]
        for k in range(depth - 1):
            differs = (lax.rem(lane - k + depth, depth) + depth - 1) // depth
            found = found + (1 - differs) * (order[k][r] - order[depth - 1][r])
        return found

    ranks = [lane] + [lane_at(r) for r in range(1, depth)]

    def piece_at(m, r, j, g):
        at = ranks[r] * inner + lax.rem(place + j, inner)
        share = lax.rem(group + g, groups) * leads + (section if leads > 1 else 0)
        start = pl.multiple_of(at * shard + share * piece, piece)
        return weights.at[m, pl.ds(start, piece)], piece_sem.at[m, at, lax.rem(group + g, groups)]

    sent = [0] * blocks

    def push(source, target, out_sem, in_sem, **where):
        pltpu.make_async_remote_copy(
            src_ref=source, dst_ref=target, send_sem=out_sem, recv_sem=in_sem, device_id=where, device_id_type=MESH
        ).start()

    def settle(like, sem):
        pltpu.make_async_copy(like, like, sem).wait()

    def settle_pieces(count, sem):
        total = count * piece
        if total <= width:
            settle(weights.at[0, pl.ds(0, total)], sem)
        else:
            settle(raw.at[pl.ds(0, total * span // width)], sem)

    def lead(step):
        if leads == 1:
            pl.when(leading)(step)
        else:
            step()

    def to_places(m, r, g):
        block, sem = piece_at(m, r, 0, g)
        for j in range(1, inner):
            push(block, block, send_sem.at[m], sem, sp=lane * inner + lax.rem(place + j, inner))
            sent[m] += 1

    def to_groups(m, r, j):
        block, sem = piece_at(m, r, j, 0)
        for g in range(1, groups):
            push(block, block, send_sem.at[m], sem, gr=lax.rem(group + g, groups))
            sent[m] += 1

    def to_sections(m, r, j, g):
        block, _ = piece_at(m, r, j, g)
        for t in range(1, sections):
            push(block, block, send_sem.at[m], cross_sem.at[m, r], tp=lax.rem(section + t, sections))
            sent[m] += 1

    def outer(m):
        return depth == 4 and OUTER[m % len(OUTER)]

    def arrive(m, r, j, g):
        settle(*piece_at(m, r, j, g))

    def step_own(m, _):
        loads[m].wait()
        lead(lambda: send_own(m))

    def send_own(m):
        block, sem = piece_at(m, 0, 0, 0)

        @pl.when(lane > 0)
        def _():
            push(block, block, send_sem.at[blocks + m], sem, sp=seat - inner)

        @pl.when(lane < depth - 1)
        def _():
            push(block, block, send_sem.at[blocks + m], sem, sp=seat + inner)

        if outer(m):
            for g in range(1, groups):
                other, its_sem = piece_at(m, 0, 0, g)
                across = lane + 1 - 2 * lax.rem(lane, 2)
                push(other, other, send_sem.at[blocks + m], its_sem, sp=across * inner + place)
        to_places(m, 0, 0)
        if CORNER[m % len(CORNER)][0] == "y":
            for g in range(1, groups):
                to_places(m, 0, g)

    def step_lane(m, r):
        arrive(m, r, 0, 0)
        block, sem = piece_at(m, r, 0, 0)
        above = (ranks[r] - lane + depth) // depth
        onward = lane + 1 - 2 * above

        @pl.when((onward >= 0) & (onward < depth))
        def _():
            push(block, block, send_sem.at[blocks + m], sem, sp=onward * inner + place)

        to_places(m, r, 0)
        if not (outer(m) and r == 1):
            to_groups(m, r, 0)
        to_sections(m, r, 0, 0)

    def corner(m, r):
        return CORNER[m % len(CORNER)][min(r, len(CORNER[0]) - 1)]

    def step_group(m, r):
        for g in range(1, groups):
            arrive(m, r, 0, g)
            if corner(m, r) == "y":
                to_places(m, r, g)
            to_sections(m, r, 0, g)

    def step_place(m, r):
        for j in range(1, inner):
            arrive(m, r, j, 0)
            if corner(m, r) == "x":
                to_groups(m, r, j)
            to_sections(m, r, j, 0)

    def step_corner(m, r):
        for j in range(1, inner):
            for g in range(1, groups):
                arrive(m, r, j, g)
                to_sections(m, r, j, g)

    filled, begun = set(), set()

    def add(m, out):
        if m in begun:
            acc[m] += out
        else:
            acc[m] = out
            begun.add(m)

    def step_norm(i, _):
        if not filled:
            smalls[0].wait()
        stage = i * norm_rows // fill_rows
        if stage not in filled:
            fills[stage].wait()
            filled.add(stage)
        step = 32

        @pl.loop(0, norm_rows // step)
        def _(k):
            here = pl.ds(pl.multiple_of(i * norm_rows + k * step, step), step)
            x = raw[here, :].astype(jnp.float32)
            mean = jnp.mean(x, axis=1, keepdims=True)
            centred = x - mean
            var = jnp.mean(centred * centred, axis=1, keepdims=True)
            scale = gain[...].astype(jnp.float32).reshape(1, width)
            normed[here, :] = (centred * lax.rsqrt(var + epsilon) * scale).astype(jnp.bfloat16)

    def crossed(m, r):
        count = ((inner - 1) if r == 0 else inner) * groups * (sections - 1 if leads > 1 else 1)
        if count and sections > 1:
            if leads > 1:
                settle_pieces(count, cross_sem.at[m, r])
            else:
                pl.when(section != sections - 1)(lambda: settle_pieces(count, cross_sem.at[m, r]))

    def step_pair(k, r):
        crossed(2 * k, r)
        crossed(2 * k + 1, r)
        long = inner * shard
        start = pl.multiple_of(ranks[r] * long, long)
        both = jnp.concatenate([weights[2 * k, pl.ds(start, long), :], weights[2 * k + 1, pl.ds(start, long), :]], axis=1)
        out = jnp.dot(normed[:, pl.ds(start, long)], both, preferred_element_type=jnp.float32)
        for m in range(2):
            add(2 * k + m, out[:, m * span:(m + 1) * span])

    def step_times(m, r):
        crossed(m, r)
        long = inner * shard
        start = pl.multiple_of(ranks[r] * long, long)
        out = jnp.dot(normed[:, pl.ds(start, long)], weights[m, pl.ds(start, long), :], preferred_element_type=jnp.float32)
        add(m, out)

    def step_trade(m, _):
        kind, part = m // per_kind, m % per_kind
        for seq in range(seqs):
            for i in range(per_block):
                cut = slice(i * head_size, (i + 1) * head_size)
                first = acc[m, seq * sub:seq * sub + half, cut]
                second = acc[m, seq * sub + half:(seq + 1) * sub, cut]
                outgoing[m, seq * per_block + i] = jnp.concatenate([first, second], axis=1).astype(jnp.bfloat16)
        home = seat // kv_heads
        for s in range(seqs):
            seq = lax.rem(home + 1 + s, seqs)
            for i in range(per_block):
                to = seq * kv_heads + part * per_block + i
                at = seq * per_block + i

                def send():
                    push(outgoing.at[m, at], incoming.at[kind, seat], last_sem.at[kind], last_sem.at[2 + kind], sp=to)

                if s < seqs - 1:
                    send()
                else:
                    pl.when(to != seat)(send)

                    @pl.when(to == seat)
                    def _():
                        incoming[kind, pl.ds(seat, 1)] = outgoing[m, pl.ds(at, 1)]

    pl.semaphore_wait(barrier, inner + groups + sections - 3 + (lane + depth - 1) // depth + (2 * depth - 2 - lane) // depth)
    calls = (step_norm, step_own, step_lane, step_group, step_place, step_corner, step_times, step_pair, step_trade)
    for which, m, r in plan(blocks, depth):
        with jax.named_scope(f"{calls[which].__name__}_{m}_{r}"):
            if HOP <= which <= EDGE:
                lead(lambda: calls[which](m, r))
            else:
                calls[which](m, r)

    for copy in smalls[1:]:
        copy.wait()
    query = queries[...].astype(jnp.float32)
    query = jnp.concatenate([query[:, g * head_size:(g + 1) * head_size] for g in range(heads)], axis=0)
    blank = jnp.zeros_like(query)
    query = jnp.concatenate(
        [jnp.concatenate([query, blank], axis=1), jnp.concatenate([blank, query], axis=1)], axis=0
    ).astype(jnp.bfloat16)
    mine = lax.broadcasted_iota(jnp.int32, (kv_heads, heads), 0) == lax.rem(seat, kv_heads)
    shift = jnp.sum(jnp.where(mine, head_shift[...], 0.0), axis=0, keepdims=True)
    eye = lax.broadcasted_iota(jnp.int32, (heads, heads), 0) == lax.broadcasted_iota(jnp.int32, (heads, heads), 1)
    shift = jnp.sum(jnp.where(eye, jnp.broadcast_to(shift, (heads, heads)), 0.0), axis=1, keepdims=True)
    later = (
        lax.broadcasted_iota(jnp.int32, (half, half), 0) > lax.broadcasted_iota(jnp.int32, (half, half), 1)
    ).astype(jnp.float32)

    with jax.named_scope("keys_in"):
        settle(incoming.at[0, pl.ds(0, seats - 1)], last_sem.at[2])
    trace = jax.named_scope("logits")
    trace.__enter__()
    keys = incoming[0].reshape(seats * half, 2 * head_size)
    logits = lax.dot_general(query, keys, (((1,), (1,)), ((), ())), preferred_element_type=jnp.float32)
    logits = logits * head_size ** (-0.5)
    betas, keeps = [], []
    for at in range(2 * seats):
        q, h = at // 2, at % 2
        z = logits[h * heads:(h + 1) * heads, q * half:(q + 1) * half]
        z = z + shift + key_shift[:, at * half:(at + 1) * half]
        tail = jnp.log1p(jnp.exp(-jnp.abs(z)))
        betas.append(jnp.minimum(z, 0.0) - tail)
        keeps.append(jnp.minimum(-z, 0.0) - tail)
    within = jnp.dot(
        jnp.concatenate(keeps, axis=0), later, preferred_element_type=jnp.float32, precision=lax.Precision.HIGHEST
    )
    running = jnp.zeros((heads, 1), jnp.float32)
    local = [None] * (2 * seats)
    for at in reversed(range(2 * seats)):
        local[at] = jnp.exp(betas[at] + within[at * heads:(at + 1) * heads] + running)
        running = running + jnp.sum(keeps[at], axis=1, keepdims=True)
    local = jnp.concatenate(
        [jnp.concatenate(local[0::2], axis=1), jnp.concatenate(local[1::2], axis=1)], axis=0
    ).astype(jnp.bfloat16)
    totals[section] = jnp.broadcast_to(running, totals.shape[1:])
    for t in range(1, sections):
        push(totals.at[section], totals.at[section], last_sem.at[4], last_sem.at[5], tp=lax.rem(section + t, sections))
    trace.__exit__(None, None, None)
    trace = jax.named_scope("totals_in")
    trace.__enter__()
    if sections > 1:
        settle(totals.at[pl.ds(0, sections - 1)], last_sem.at[5])
    carry = jnp.zeros((heads, head_size), jnp.float32)
    for t in reversed(range(sections)):
        carry = carry + jnp.where(section < t, totals[t][:, :head_size], 0.0)
    carry = jnp.exp(carry)
    trace.__exit__(None, None, None)

    with jax.named_scope("values_in"):
        settle(incoming.at[1, pl.ds(0, seats - 1)], last_sem.at[3])
    trace = jax.named_scope("part")
    trace.__enter__()
    values = incoming[1].reshape(seats * half, 2 * head_size)
    part = jnp.dot(local, values, preferred_element_type=jnp.float32)
    part = carry * (part[:heads, :head_size] + part[heads:, head_size:])
    parts[section] = jnp.concatenate([part, part], axis=1)
    for t in range(1, sections):
        push(parts.at[section], parts.at[section], last_sem.at[6], last_sem.at[7], tp=lax.rem(section + t, sections))
    trace.__exit__(None, None, None)
    trace = jax.named_scope("cache")
    trace.__enter__()
    for q in range(seats):
        for h in range(2):
            cut = slice(h * head_size, (h + 1) * head_size)
            start = (2 * q + h) * half
            cache[0, start:start + half, :] = jnp.concatenate([incoming[0, q][:, cut], incoming[1, q][:, cut]], axis=1)
    def drain():
        for m in range(blocks):
            settle_pieces(sent[m], send_sem.at[m])
            for k in range(depth):
                count = (k + 1 if k < depth - 1 else 0) + (depth - k if k > 0 else 0) + (groups - 1) * outer(m)
                if count:
                    pl.when(lane == k)(lambda count=count: settle_pieces(count, send_sem.at[blocks + m]))

    lead(drain)
    for kind in range(2):
        settle(incoming.at[kind, pl.ds(0, seats - 1)], last_sem.at[kind])
    trace.__exit__(None, None, None)
    trace = jax.named_scope("parts_in")
    trace.__enter__()
    if sections > 1:
        settle(totals.at[pl.ds(0, sections - 1)], last_sem.at[4])
        settle(parts.at[pl.ds(0, sections - 1)], last_sem.at[6])
        settle(parts.at[pl.ds(0, sections - 1)], last_sem.at[7])
    total = parts[0]
    for t in range(1, sections):
        total = total + parts[t]
    for g in range(heads):
        read[:, g * head_size:(g + 1) * head_size] = total[g:g + 1, :head_size]
    trace.__exit__(None, None, None)


def hand_over(cache, read, cache_out, read_out, sem):
    first = pltpu.make_async_copy(cache, cache_out, sem.at[0])
    second = pltpu.make_async_copy(read, read_out, sem.at[1])
    first.start()
    second.start()
    first.wait()
    second.wait()


def local(grid, tokens, ln_gain, w_key, w_value, queries, head_shift, key_shift):
    depth, inner, groups, sections = grid
    seats = depth * inner
    seqs, _, sub, width = tokens.shape
    rows = seqs * sub
    columns = w_key.shape[1]
    kv_heads, heads = head_shift.shape
    head_size = columns // kv_heads
    blocks = 2 * columns // LANES
    vmem = pl.BlockSpec(memory_space=pltpu.VMEM)
    hbm = pl.BlockSpec(memory_space=pl.ANY)
    operands = (tokens.reshape(rows, width), ln_gain, w_key, w_value, queries, head_shift, key_shift)
    cache, read = pl.pallas_call(
        functools.partial(body, grid, head_size),
        out_shape=(
            jax.ShapeDtypeStruct((1, seats * sub, 2 * head_size), jnp.bfloat16),
            jax.ShapeDtypeStruct((1, heads * head_size), jnp.float32),
        ),
        in_specs=[hbm] * len(operands),
        out_specs=(vmem, vmem),
        scratch_shapes=[
            pltpu.VMEM((rows, width), jnp.bfloat16),
            pltpu.VMEM((rows, width), jnp.bfloat16),
            pltpu.VMEM((blocks, width, LANES), jnp.bfloat16),
            pltpu.VMEM((blocks, rows, LANES), jnp.float32),
            pltpu.VMEM((blocks, seqs * LANES // head_size, sub // 2, 2 * head_size), jnp.bfloat16),
            pltpu.VMEM((2, seats, sub // 2, 2 * head_size), jnp.bfloat16),
            pltpu.VMEM((sections, heads, 2 * head_size), jnp.float32),
            pltpu.VMEM((sections, heads, 2 * head_size), jnp.float32),
            pltpu.VMEM(ln_gain.shape, ln_gain.dtype),
            pltpu.VMEM(queries.shape, queries.dtype),
            pltpu.VMEM(head_shift.shape, head_shift.dtype),
            pltpu.VMEM(key_shift.shape, key_shift.dtype),
            pltpu.SemaphoreType.DMA((2 * blocks,)),
            pltpu.SemaphoreType.DMA((blocks, seats, groups)),
            pltpu.SemaphoreType.DMA((blocks, depth)),
            pltpu.SemaphoreType.DMA((8,)),
            pltpu.SemaphoreType.DMA((blocks + FILLS + 4,)),
        ],
        compiler_params=pltpu.CompilerParams(
            collective_id=0, has_side_effects=True, vmem_limit_bytes=24 * 1024 * 1024
        ),
    )(*(pltpu.with_memory_space_constraint(x, pltpu.HBM) for x in operands))
    return pl.pallas_call(
        hand_over,
        out_shape=(jax.ShapeDtypeStruct(cache.shape, cache.dtype), jax.ShapeDtypeStruct(read.shape, read.dtype)),
        in_specs=[vmem, vmem],
        out_specs=(hbm, hbm),
        scratch_shapes=[pltpu.SemaphoreType.DMA((2,))],
        compiler_params=pltpu.CompilerParams(vmem_limit_bytes=4 * 1024 * 1024),
    )(cache, read)


def solution(mesh):
    in_specs = (
        P("gr", "tp", "sp", None),
        P(),
        P("sp", None),
        P("sp", None),
        P(("gr", "sp"), None),
        P(),
        P(("gr", "sp"), "tp"),
    )
    out_specs = (P(("gr", "sp"), "tp", None), P(("gr", "sp"), None))
    return jax.shard_map(
        functools.partial(local, layout(mesh)), mesh=mesh, in_specs=in_specs, out_specs=out_specs, check_vma=False
    )
```

```python
import functools

import jax
import jax.numpy as jnp
from jax import lax
from jax.experimental import pallas as pl
from jax.experimental.pallas import tpu as pltpu
from jax.sharding import PartitionSpec as P

epsilon = 1e-05
LANES = 128
NORM, OWN, HOP, GROUP, PLACE, EDGE, TIMES, PAIR, TRADE = range(9)
FILLS = 4
NORMS = 8
BASES = (0.0, 2.0, 4.0, 6.0)
LANE_STEP, GROUP_AT, PLACE_AT, CORNER_AT, TIMES_AT, OWN_AT = 1.5, 3.0, 2.0, 5.0, 7.0, -3.0
NORM_START, NORM_STEP = 0.2, 0.6
CORNER = (("x", "x", "x", "y"), ("y", "x", "y", "x"), ("x", "x", "y", "y"), ("x", "x", "y", "x"))
OUTER = (False, False, True, True)
ORDER = (
    (OWN, 0, 0), (OWN, 1, 0), (NORM, 2, 0), (OWN, 3, 0), (OWN, 2, 0), (NORM, 7, 0),
    (HOP, 0, 1), (HOP, 1, 1), (PLACE, 0, 0), (PLACE, 1, 0), (HOP, 0, 2), (NORM, 6, 0),
    (HOP, 2, 2), (HOP, 1, 2), (HOP, 0, 3), (PLACE, 0, 1), (HOP, 2, 1), (NORM, 0, 0),
    (PLACE, 1, 1), (HOP, 3, 1), (HOP, 1, 3), (EDGE, 1, 0), (GROUP, 1, 1), (PLACE, 0, 2),
    (HOP, 3, 2), (PLACE, 2, 2), (NORM, 4, 0), (GROUP, 2, 1), (NORM, 3, 0), (GROUP, 0, 1),
    (GROUP, 0, 3), (HOP, 3, 3), (NORM, 1, 0), (NORM, 5, 0), (HOP, 2, 3), (EDGE, 0, 1),
    (PLACE, 1, 3), (EDGE, 1, 1), (TIMES, 1, 1), (GROUP, 0, 2), (GROUP, 1, 2), (TIMES, 0, 1),
    (PLACE, 3, 2), (PLACE, 2, 0), (EDGE, 0, 0), (TIMES, 0, 0), (PLACE, 1, 2), (PLACE, 2, 1),
    (PLACE, 0, 3), (GROUP, 3, 1), (GROUP, 2, 2), (EDGE, 0, 2), (TIMES, 0, 2), (GROUP, 1, 3),
    (EDGE, 0, 3), (PLACE, 3, 0), (TIMES, 0, 3), (TRADE, 0, 0), (TIMES, 1, 0), (GROUP, 2, 3),
    (PLACE, 3, 1), (PLACE, 2, 3), (EDGE, 1, 3), (TIMES, 1, 3), (PLACE, 3, 3), (EDGE, 1, 2),
    (TIMES, 1, 2), (EDGE, 2, 2), (EDGE, 2, 0), (TIMES, 2, 0), (TRADE, 1, 0), (EDGE, 2, 1),
    (TIMES, 2, 1), (EDGE, 3, 0), (TIMES, 3, 0), (GROUP, 3, 2), (EDGE, 3, 1), (TIMES, 2, 2),
    (EDGE, 2, 3), (TIMES, 2, 3), (TRADE, 2, 0), (TIMES, 3, 1), (EDGE, 3, 2), (TIMES, 3, 2),
    (GROUP, 3, 3), (EDGE, 3, 3), (TIMES, 3, 3), (TRADE, 3, 0),
)
MESH = pl.DeviceIdType.MESH


def layout(mesh):
    sp, gr, tp = mesh.shape["sp"], mesh.shape["gr"], mesh.shape["tp"]
    inner = 1
    while inner * inner * 4 <= sp and sp % (inner * 2) == 0:
        inner *= 2
    return sp // inner, inner, gr, tp


def nearest(depth):
    return [[lane] + sorted((k for k in range(depth) if k != lane), key=lambda k: (abs(k - lane), k if 2 * lane < depth else -k)) for lane in range(depth)]


def plan(blocks, depth):
    if (blocks, depth) == (len(CORNER), len(CORNER[0])):
        return ORDER
    steps = []
    for i in range(NORMS):
        steps.append((NORM_START + i * NORM_STEP, NORM, i, 0))
    for m in range(blocks):
        base = BASES[m % len(BASES)]
        steps.append((base + OWN_AT, OWN, m, 0))
        for r in range(depth):
            at = base + r * LANE_STEP
            if r:
                steps.append((at, HOP, m, r))
                steps.append((at + GROUP_AT, GROUP, m, r))
            steps.append((at + PLACE_AT, PLACE, m, r))
            steps.append((at + CORNER_AT, EDGE, m, r))
            end = max(at + TIMES_AT, NORM_START + NORMS * NORM_STEP)
            steps.append((end, TIMES, m, r))
        steps.append((end + 0.001, TRADE, m, 0))
    return [step[1:] for step in sorted(steps, key=lambda step: step[0])]


def body(
    grid, head_size,
    tokens, gain_in, w_key, w_value, queries_in, head_shift_in, key_shift_in,
    cache, read,
    raw, normed, weights, acc, outgoing, incoming, parts,
    gain, queries, head_shift, key_shift,
    send_sem, piece_sem, cross_sem, last_sem, load_sem,
):
    depth, inner, groups, sections = grid
    seats = depth * inner
    seat, group, section = lax.axis_index("sp"), lax.axis_index("gr"), lax.axis_index("tp")
    lane, place = seat // inner, seat % inner
    rows, width = raw.shape
    shard, columns = w_key.shape
    blocks, _, span = weights.shape
    leads = sections if sections > 2 else 1
    leading = section == sections - 1
    merged = 2 if leads == 1 else 1
    piece = shard // (groups * leads)
    kv_heads, heads = head_shift.shape
    seqs = seats // kv_heads
    sub = rows // seqs
    half = sub // 2
    per_kind = columns // span
    per_block = span // head_size
    fill_rows = rows // FILLS
    norm_rows = rows // NORMS

    own = pl.ds(pl.multiple_of(seat * shard, shard), shard)
    loads = []
    for m in range(blocks):
        source = (w_key, w_value)[m // per_kind].at[:, pl.ds((m % per_kind) * span, span)]
        loads.append(pltpu.make_async_copy(source, weights.at[m, own], load_sem.at[m]))
        loads[-1].start()
    fills = []
    for at in range(FILLS):
        rows_at = pl.ds(at * fill_rows, fill_rows)
        fills.append(pltpu.make_async_copy(tokens.at[rows_at], raw.at[rows_at], load_sem.at[blocks + at]))
        fills[-1].start()
    smalls = []
    for at, (source, target) in enumerate(
        ((gain_in, gain), (queries_in, queries), (head_shift_in, head_shift), (key_shift_in, key_shift))
    ):
        smalls.append(pltpu.make_async_copy(source, target, load_sem.at[blocks + FILLS + at]))
        smalls[-1].start()

    barrier = pltpu.get_barrier_semaphore()

    def greet(**where):
        pl.semaphore_signal(barrier, 1, device_id=where, device_id_type=MESH)

    @pl.when(lane > 0)
    def _():
        greet(sp=seat - inner)

    @pl.when(lane < depth - 1)
    def _():
        greet(sp=seat + inner)

    for j in range(1, inner):
        greet(sp=lane * inner + lax.rem(place + j, inner))
    for g in range(1, groups):
        greet(gr=lax.rem(group + g, groups))
    for t in range(1, sections):
        greet(tp=lax.rem(section + t, sections))

    order = nearest(depth)

    def lane_at(r):
        found = order[depth - 1][r]
        for k in range(depth - 1):
            differs = (lax.rem(lane - k + depth, depth) + depth - 1) // depth
            found = found + (1 - differs) * (order[k][r] - order[depth - 1][r])
        return found

    ranks = [lane] + [lane_at(r) for r in range(1, depth)]

    def piece_at(m, r, j, g):
        at = ranks[r] * inner + lax.rem(place + j, inner)
        share = lax.rem(group + g, groups) * leads + (section if leads > 1 else 0)
        start = pl.multiple_of(at * shard + share * piece, piece)
        return weights.at[m, pl.ds(start, piece)], piece_sem.at[m, at, lax.rem(group + g, groups)]

    sent = [0] * blocks

    def push(source, target, out_sem, in_sem, **where):
        pltpu.make_async_remote_copy(
            src_ref=source, dst_ref=target, send_sem=out_sem, recv_sem=in_sem, device_id=where, device_id_type=MESH
        ).start()

    def settle(like, sem):
        pltpu.make_async_copy(like, like, sem).wait()

    def settle_pieces(count, sem):
        total = count * piece
        if total <= width:
            settle(weights.at[0, pl.ds(0, total)], sem)
        else:
            settle(raw.at[pl.ds(0, total * span // width)], sem)

    def lead(step):
        if leads == 1:
            pl.when(leading)(step)
        else:
            step()

    def to_places(m, r, g):
        block, sem = piece_at(m, r, 0, g)
        for j in range(1, inner):
            push(block, block, send_sem.at[m // merged], sem, sp=lane * inner + lax.rem(place + j, inner))
            sent[m] += 1

    def to_groups(m, r, j):
        block, sem = piece_at(m, r, j, 0)
        for g in range(1, groups):
            push(block, block, send_sem.at[m // merged], sem, gr=lax.rem(group + g, groups))
            sent[m] += 1

    def to_sections(m, r, j, g):
        block, _ = piece_at(m, r, j, g)
        for t in range(1, sections):
            push(block, block, send_sem.at[m // merged], cross_sem.at[m, r], tp=lax.rem(section + t, sections))
            sent[m] += 1

    def outer(m):
        return depth == 4 and OUTER[m % len(OUTER)]

    def arrive(m, r, j, g):
        settle(*piece_at(m, r, j, g))

    def step_own(m, _):
        loads[m].wait()
        lead(lambda: send_own(m))

    def send_own(m):
        block, sem = piece_at(m, 0, 0, 0)

        @pl.when(lane > 0)
        def _():
            push(block, block, send_sem.at[m // merged], sem, sp=seat - inner)

        @pl.when(lane < depth - 1)
        def _():
            push(block, block, send_sem.at[m // merged], sem, sp=seat + inner)

        if outer(m):
            for g in range(1, groups):
                other, its_sem = piece_at(m, 0, 0, g)
                across = lane + 1 - 2 * lax.rem(lane, 2)
                push(other, other, send_sem.at[m // merged], its_sem, sp=across * inner + place)
        to_places(m, 0, 0)
        if CORNER[m % len(CORNER)][0] == "y":
            for g in range(1, groups):
                to_places(m, 0, g)

    def step_lane(m, r):
        arrive(m, r, 0, 0)
        block, sem = piece_at(m, r, 0, 0)
        above = (ranks[r] - lane + depth) // depth
        onward = lane + 1 - 2 * above

        @pl.when((onward >= 0) & (onward < depth))
        def _():
            push(block, block, send_sem.at[m // merged], sem, sp=onward * inner + place)

        to_places(m, r, 0)
        if not (outer(m) and r == 1):
            to_groups(m, r, 0)
        to_sections(m, r, 0, 0)

    def corner(m, r):
        return CORNER[m % len(CORNER)][min(r, len(CORNER[0]) - 1)]

    def step_group(m, r):
        for g in range(1, groups):
            arrive(m, r, 0, g)
            if corner(m, r) == "y":
                to_places(m, r, g)
            to_sections(m, r, 0, g)

    def step_place(m, r):
        for j in range(1, inner):
            arrive(m, r, j, 0)
            if corner(m, r) == "x":
                to_groups(m, r, j)
            to_sections(m, r, j, 0)

    def step_corner(m, r):
        for j in range(1, inner):
            for g in range(1, groups):
                arrive(m, r, j, g)
                to_sections(m, r, j, g)

    filled, begun = set(), set()

    def add(m, out):
        if m in begun:
            acc[m] += out
        else:
            acc[m] = out
            begun.add(m)

    def step_norm(i, _):
        if not filled:
            smalls[0].wait()
        stage = i * norm_rows // fill_rows
        if stage not in filled:
            fills[stage].wait()
            filled.add(stage)
        step = 32

        @pl.loop(0, norm_rows // step)
        def _(k):
            here = pl.ds(pl.multiple_of(i * norm_rows + k * step, step), step)
            x = raw[here, :].astype(jnp.float32)
            mean = jnp.mean(x, axis=1, keepdims=True)
            centred = x - mean
            var = jnp.mean(centred * centred, axis=1, keepdims=True)
            scale = gain[...].astype(jnp.float32).reshape(1, width)
            normed[here, :] = (centred * lax.rsqrt(var + epsilon) * scale).astype(jnp.bfloat16)

    def crossed(m, r):
        count = ((inner - 1) if r == 0 else inner) * groups * (sections - 1 if leads > 1 else 1)
        if count and sections > 1:
            if leads > 1:
                settle_pieces(count, cross_sem.at[m, r])
            else:
                pl.when(section != sections - 1)(lambda: settle_pieces(count, cross_sem.at[m, r]))

    def step_pair(k, r):
        crossed(2 * k, r)
        crossed(2 * k + 1, r)
        long = inner * shard
        start = pl.multiple_of(ranks[r] * long, long)
        both = jnp.concatenate([weights[2 * k, pl.ds(start, long), :], weights[2 * k + 1, pl.ds(start, long), :]], axis=1)
        out = jnp.dot(normed[:, pl.ds(start, long)], both, preferred_element_type=jnp.float32)
        for m in range(2):
            add(2 * k + m, out[:, m * span:(m + 1) * span].T)

    def step_times(m, r):
        crossed(m, r)
        long = inner * shard
        start = pl.multiple_of(ranks[r] * long, long)
        add(m, lax.dot_general(
            weights[m, pl.ds(start, long), :], normed[:, pl.ds(start, long)], (((0,), (1,)), ((), ())),
            preferred_element_type=jnp.float32,
        ))

    def step_trade(m, _):
        kind, part = m // per_kind, m % per_kind
        block = acc[m].T
        for seq in range(seqs):
            for i in range(per_block):
                cut = slice(i * head_size, (i + 1) * head_size)
                first = block[seq * sub:seq * sub + half, cut]
                second = block[seq * sub + half:(seq + 1) * sub, cut]
                outgoing[m, seq * per_block + i] = jnp.concatenate([first, second], axis=1).astype(jnp.bfloat16)
        for seq in range(seqs):
            for i in range(per_block):
                to = seq * kv_heads + part * per_block + i
                at = seq * per_block + i

                @pl.when(seat != to)
                def _():
                    push(outgoing.at[m, at], incoming.at[kind, seat], last_sem.at[kind], last_sem.at[2 + kind], sp=to)

                @pl.when(seat == to)
                def _():
                    incoming[kind, to] = outgoing[m, at]

    pl.semaphore_wait(barrier, inner + groups + sections - 3 + (lane + depth - 1) // depth + (2 * depth - 2 - lane) // depth)
    calls = (step_norm, step_own, step_lane, step_group, step_place, step_corner, step_times, step_pair, step_trade)
    for which, m, r in plan(blocks, depth):
        with jax.named_scope(f"{calls[which].__name__}_{m}_{r}"):
            if HOP <= which <= EDGE:
                lead(lambda: calls[which](m, r))
            else:
                calls[which](m, r)

    for copy in smalls[1:]:
        copy.wait()
    query = queries[...].astype(jnp.float32)
    query = jnp.concatenate([query[:, g * head_size:(g + 1) * head_size] for g in range(heads)], axis=0)
    blank = jnp.zeros_like(query)
    query = jnp.concatenate(
        [jnp.concatenate([query, blank], axis=1), jnp.concatenate([blank, query], axis=1)], axis=0
    ).astype(jnp.bfloat16)
    mine = lax.broadcasted_iota(jnp.int32, (kv_heads, heads), 0) == lax.rem(seat, kv_heads)
    shift = jnp.sum(jnp.where(mine, head_shift[...], 0.0), axis=0, keepdims=True)
    eye = lax.broadcasted_iota(jnp.int32, (heads, heads), 0) == lax.broadcasted_iota(jnp.int32, (heads, heads), 1)
    shift = jnp.sum(jnp.where(eye, jnp.broadcast_to(shift, (heads, heads)), 0.0), axis=1, keepdims=True)
    later = (
        lax.broadcasted_iota(jnp.int32, (half, half), 0) > lax.broadcasted_iota(jnp.int32, (half, half), 1)
    ).astype(jnp.float32)

    with jax.named_scope("keys_in"):
        settle(incoming.at[0, pl.ds(0, seats - 1)], last_sem.at[2])
    trace = jax.named_scope("logits")
    trace.__enter__()
    keys = incoming[0].reshape(seats * half, 2 * head_size)
    logits = lax.dot_general(query, keys, (((1,), (1,)), ((), ())), preferred_element_type=jnp.float32)
    logits = logits * head_size ** (-0.5)
    betas, keeps = [], []
    for at in range(2 * seats):
        q, h = at // 2, at % 2
        z = logits[h * heads:(h + 1) * heads, q * half:(q + 1) * half]
        z = z + shift + key_shift[:, at * half:(at + 1) * half]
        tail = jnp.log1p(jnp.exp(-jnp.abs(z)))
        betas.append(jnp.minimum(z, 0.0) - tail)
        keeps.append(jnp.minimum(-z, 0.0) - tail)
    within = jnp.dot(
        jnp.concatenate(keeps, axis=0), later, preferred_element_type=jnp.float32, precision=lax.Precision.HIGHEST
    )
    running = jnp.zeros((heads, 1), jnp.float32)
    local = [None] * (2 * seats)
    for at in reversed(range(2 * seats)):
        local[at] = jnp.exp(betas[at] + within[at * heads:(at + 1) * heads] + running)
        running = running + jnp.sum(keeps[at], axis=1, keepdims=True)
    local = jnp.concatenate(
        [jnp.concatenate(local[0::2], axis=1), jnp.concatenate(local[1::2], axis=1)], axis=0
    ).astype(jnp.bfloat16)
    trace.__exit__(None, None, None)
    with jax.named_scope("values_in"):
        settle(incoming.at[1, pl.ds(0, seats - 1)], last_sem.at[3])
    trace = jax.named_scope("part")
    trace.__enter__()
    values = incoming[1].reshape(seats * half, 2 * head_size)
    part = jnp.dot(local, values, preferred_element_type=jnp.float32)
    part = part[:heads, :head_size] + part[heads:, head_size:]
    parts[section] = jnp.concatenate([part, jnp.broadcast_to(running, part.shape)], axis=1)
    for t in range(1, sections):
        push(parts.at[section], parts.at[section], last_sem.at[4], last_sem.at[5], tp=lax.rem(section + t, sections))
    trace.__exit__(None, None, None)
    trace = jax.named_scope("cache")
    trace.__enter__()
    for q in range(seats):
        for h in range(2):
            cut = slice(h * head_size, (h + 1) * head_size)
            start = (2 * q + h) * half
            cache[0, start:start + half, :] = jnp.concatenate([incoming[0, q][:, cut], incoming[1, q][:, cut]], axis=1)
    def drain():
        for pair in range(blocks // merged):
            both = range(merged * pair, merged * (pair + 1))
            for k in range(depth):
                count = sum(sent[m] + (k + 1) * (k < depth - 1) + (depth - k) * (k > 0) + (groups - 1) * outer(m) for m in both)
                pl.when(lane == k)(lambda count=count: settle_pieces(count, send_sem.at[pair]))

    lead(drain)
    for kind in range(2):
        settle(incoming.at[kind, pl.ds(0, seats - 1)], last_sem.at[kind])
    trace.__exit__(None, None, None)
    trace = jax.named_scope("parts_in")
    trace.__enter__()
    if sections > 1:
        settle(parts.at[pl.ds(0, sections - 1)], last_sem.at[4])
        settle(parts.at[pl.ds(0, sections - 1)], last_sem.at[5])
    total = jnp.zeros((heads, head_size), jnp.float32)
    carry = jnp.zeros((heads, head_size), jnp.float32)
    for t in reversed(range(sections)):
        total = total + jnp.exp(carry) * parts[t][:, :head_size]
        carry = carry + parts[t][:, head_size:]
    for g in range(heads):
        read[:, g * head_size:(g + 1) * head_size] = total[g:g + 1, :]
    trace.__exit__(None, None, None)


def hand_over(cache, read, cache_out, read_out, sem):
    first = pltpu.make_async_copy(cache, cache_out, sem.at[0])
    second = pltpu.make_async_copy(read, read_out, sem.at[1])
    first.start()
    second.start()
    first.wait()
    second.wait()


def local(grid, tokens, ln_gain, w_key, w_value, queries, head_shift, key_shift):
    depth, inner, groups, sections = grid
    seats = depth * inner
    seqs, _, sub, width = tokens.shape
    rows = seqs * sub
    columns = w_key.shape[1]
    kv_heads, heads = head_shift.shape
    head_size = columns // kv_heads
    blocks = 2 * columns // LANES
    vmem = pl.BlockSpec(memory_space=pltpu.VMEM)
    hbm = pl.BlockSpec(memory_space=pl.ANY)
    operands = (tokens.reshape(rows, width), ln_gain, w_key, w_value, queries, head_shift, key_shift)
    cache, read = pl.pallas_call(
        functools.partial(body, grid, head_size),
        out_shape=(
            jax.ShapeDtypeStruct((1, seats * sub, 2 * head_size), jnp.bfloat16),
            jax.ShapeDtypeStruct((1, heads * head_size), jnp.float32),
        ),
        in_specs=[hbm] * len(operands),
        out_specs=(vmem, vmem),
        scratch_shapes=[
            pltpu.VMEM((rows, width), jnp.bfloat16),
            pltpu.VMEM((rows, width), jnp.bfloat16),
            pltpu.VMEM((blocks, width, LANES), jnp.bfloat16),
            pltpu.VMEM((blocks, LANES, rows), jnp.float32),
            pltpu.VMEM((blocks, seqs * LANES // head_size, sub // 2, 2 * head_size), jnp.bfloat16),
            pltpu.VMEM((2, seats, sub // 2, 2 * head_size), jnp.bfloat16),
            pltpu.VMEM((sections, heads, 2 * head_size), jnp.float32),
            pltpu.VMEM(ln_gain.shape, ln_gain.dtype),
            pltpu.VMEM(queries.shape, queries.dtype),
            pltpu.VMEM(head_shift.shape, head_shift.dtype),
            pltpu.VMEM(key_shift.shape, key_shift.dtype),
            pltpu.SemaphoreType.DMA((blocks,)),
            pltpu.SemaphoreType.DMA((blocks, seats, groups)),
            pltpu.SemaphoreType.DMA((blocks, depth)),
            pltpu.SemaphoreType.DMA((6,)),
            pltpu.SemaphoreType.DMA((blocks + FILLS + 4,)),
        ],
        compiler_params=pltpu.CompilerParams(
            collective_id=0, has_side_effects=True, vmem_limit_bytes=24 * 1024 * 1024
        ),
    )(*(pltpu.with_memory_space_constraint(x, pltpu.HBM) for x in operands))
    return pl.pallas_call(
        hand_over,
        out_shape=(jax.ShapeDtypeStruct(cache.shape, cache.dtype), jax.ShapeDtypeStruct(read.shape, read.dtype)),
        in_specs=[vmem, vmem],
        out_specs=(hbm, hbm),
        scratch_shapes=[pltpu.SemaphoreType.DMA((2,))],
        compiler_params=pltpu.CompilerParams(vmem_limit_bytes=4 * 1024 * 1024),
    )(cache, read)


def solution(mesh):
    in_specs = (
        P("gr", "tp", "sp", None),
        P(),
        P("sp", None),
        P("sp", None),
        P(("gr", "sp"), None),
        P(),
        P(("gr", "sp"), "tp"),
    )
    out_specs = (P(("gr", "sp"), "tp", None), P(("gr", "sp"), None))
    return jax.shard_map(
        functools.partial(local, layout(mesh)), mesh=mesh, in_specs=in_specs, out_specs=out_specs, check_vma=False
    )
```

```python
import functools

import jax
import jax.numpy as jnp
from jax import lax
from jax.experimental import pallas as pl
from jax.experimental.pallas import tpu as pltpu
from jax.sharding import PartitionSpec as P

epsilon = 1e-05
LANES = 128
NORM, OWN, HOP, GROUP, PLACE, EDGE, TIMES, PAIR, TRADE = range(9)
FILLS = 1
NORMS = 8
BASES = (0.0, 2.0, 4.0, 6.0)
LANE_STEP, GROUP_AT, PLACE_AT, CORNER_AT, TIMES_AT, OWN_AT = 1.5, 3.0, 2.0, 5.0, 7.0, -3.0
NORM_START, NORM_STEP = 0.2, 0.6
CORNER = (("x", "x", "x", "y"), ("y", "x", "y", "x"), ("x", "x", "y", "y"), ("x", "x", "y", "x"))
OUTER = (False, False, True, True)
ORDER = (
    (OWN, 0, 0), (OWN, 1, 0), (NORM, 2, 0), (OWN, 3, 0), (OWN, 2, 0), (NORM, 7, 0),
    (HOP, 0, 1), (HOP, 1, 1), (PLACE, 0, 0), (PLACE, 1, 0), (HOP, 0, 2), (NORM, 6, 0),
    (HOP, 2, 2), (HOP, 1, 2), (HOP, 0, 3), (PLACE, 0, 1), (HOP, 2, 1), (NORM, 0, 0),
    (PLACE, 1, 1), (HOP, 3, 1), (HOP, 1, 3), (EDGE, 1, 0), (GROUP, 1, 1), (PLACE, 0, 2),
    (HOP, 3, 2), (PLACE, 2, 2), (NORM, 4, 0), (GROUP, 2, 1), (NORM, 3, 0), (GROUP, 0, 1),
    (GROUP, 0, 3), (HOP, 3, 3), (NORM, 1, 0), (NORM, 5, 0), (HOP, 2, 3), (EDGE, 0, 1),
    (PLACE, 1, 3), (EDGE, 1, 1), (TIMES, 1, 1), (GROUP, 0, 2), (GROUP, 1, 2), (TIMES, 0, 1),
    (PLACE, 3, 2), (PLACE, 2, 0), (EDGE, 0, 0), (TIMES, 0, 0), (PLACE, 1, 2), (PLACE, 2, 1),
    (PLACE, 0, 3), (GROUP, 3, 1), (GROUP, 2, 2), (EDGE, 0, 2), (TIMES, 0, 2), (GROUP, 1, 3),
    (EDGE, 0, 3), (PLACE, 3, 0), (TIMES, 0, 3), (TRADE, 0, 0), (TIMES, 1, 0), (GROUP, 2, 3),
    (PLACE, 3, 1), (PLACE, 2, 3), (EDGE, 1, 3), (TIMES, 1, 3), (PLACE, 3, 3), (EDGE, 1, 2),
    (TIMES, 1, 2), (EDGE, 2, 2), (EDGE, 2, 0), (TIMES, 2, 0), (TRADE, 1, 0), (EDGE, 2, 1),
    (TIMES, 2, 1), (EDGE, 3, 0), (TIMES, 3, 0), (GROUP, 3, 2), (EDGE, 3, 1), (TIMES, 2, 2),
    (EDGE, 2, 3), (TIMES, 2, 3), (TRADE, 2, 0), (TIMES, 3, 1), (EDGE, 3, 2), (TIMES, 3, 2),
    (GROUP, 3, 3), (EDGE, 3, 3), (TIMES, 3, 3), (TRADE, 3, 0),
)
MESH = pl.DeviceIdType.MESH


def layout(mesh):
    sp, gr, tp = mesh.shape["sp"], mesh.shape["gr"], mesh.shape["tp"]
    inner = 1
    while inner * inner * 4 <= sp and sp % (inner * 2) == 0:
        inner *= 2
    return sp // inner, inner, gr, tp


def nearest(depth):
    return [[lane] + sorted((k for k in range(depth) if k != lane), key=lambda k: (abs(k - lane), k if 2 * lane < depth else -k)) for lane in range(depth)]


def plan(blocks, depth):
    if (blocks, depth) == (len(CORNER), len(CORNER[0])):
        return ORDER
    steps = []
    for i in range(NORMS):
        steps.append((NORM_START + i * NORM_STEP, NORM, i, 0))
    for m in range(blocks):
        base = BASES[m % len(BASES)]
        steps.append((base + OWN_AT, OWN, m, 0))
        for r in range(depth):
            at = base + r * LANE_STEP
            if r:
                steps.append((at, HOP, m, r))
                steps.append((at + GROUP_AT, GROUP, m, r))
            steps.append((at + PLACE_AT, PLACE, m, r))
            steps.append((at + CORNER_AT, EDGE, m, r))
            end = max(at + TIMES_AT, NORM_START + NORMS * NORM_STEP)
            steps.append((end, TIMES, m, r))
        steps.append((end + 0.001, TRADE, m, 0))
    return [step[1:] for step in sorted(steps, key=lambda step: step[0])]


def body(
    grid, head_size,
    tokens, gain_in, w_key, w_value, queries_in, head_shift_in, key_shift_in,
    cache, read,
    raw, normed, weights, acc, outgoing, incoming, parts,
    gain, queries, head_shift, key_shift,
    send_sem, piece_sem, cross_sem, last_sem, load_sem,
):
    depth, inner, groups, sections = grid
    seats = depth * inner
    seat, group, section = lax.axis_index("sp"), lax.axis_index("gr"), lax.axis_index("tp")
    lane, place = seat // inner, seat % inner
    rows, width = raw.shape
    shard, columns = w_key.shape
    blocks, _, span = weights.shape
    leads = sections if sections > 2 else 1
    leading = section == sections - 1
    merged = 2 if leads == 1 else 1
    piece = shard // (groups * leads)
    kv_heads, heads = head_shift.shape
    seqs = seats // kv_heads
    sub = rows // seqs
    half = sub // 2
    per_kind = columns // span
    per_block = span // head_size
    fill_rows = rows // FILLS
    norm_rows = rows // NORMS

    own = pl.ds(pl.multiple_of(seat * shard, shard), shard)
    loads = []
    for m in range(blocks):
        source = (w_key, w_value)[m // per_kind].at[:, pl.ds((m % per_kind) * span, span)]
        loads.append(pltpu.make_async_copy(source, weights.at[m, own], load_sem.at[m]))
        loads[-1].start()
    fills = []
    for at in range(FILLS):
        rows_at = pl.ds(at * fill_rows, fill_rows)
        fills.append(pltpu.make_async_copy(tokens.at[rows_at], raw.at[rows_at], load_sem.at[blocks + at]))
        fills[-1].start()
    smalls = []
    for at, (source, target) in enumerate(
        ((gain_in, gain), (queries_in, queries), (head_shift_in, head_shift), (key_shift_in, key_shift))
    ):
        smalls.append(pltpu.make_async_copy(source, target, load_sem.at[blocks + FILLS + at]))
        smalls[-1].start()

    barrier = pltpu.get_barrier_semaphore()

    def greet(**where):
        pl.semaphore_signal(barrier, 1, device_id=where, device_id_type=MESH)

    @pl.when(lane > 0)
    def _():
        greet(sp=seat - inner)

    @pl.when(lane < depth - 1)
    def _():
        greet(sp=seat + inner)

    for j in range(1, inner):
        greet(sp=lane * inner + lax.rem(place + j, inner))
    for g in range(1, groups):
        greet(gr=lax.rem(group + g, groups))
    for t in range(1, sections):
        greet(tp=lax.rem(section + t, sections))

    order = nearest(depth)

    def lane_at(r):
        found = order[depth - 1][r]
        for k in range(depth - 1):
            differs = (lax.rem(lane - k + depth, depth) + depth - 1) // depth
            found = found + (1 - differs) * (order[k][r] - order[depth - 1][r])
        return found

    ranks = [lane] + [lane_at(r) for r in range(1, depth)]

    def piece_at(m, r, j, g):
        at = ranks[r] * inner + lax.rem(place + j, inner)
        share = lax.rem(group + g, groups) * leads + (section if leads > 1 else 0)
        start = pl.multiple_of(at * shard + share * piece, piece)
        return weights.at[m, pl.ds(start, piece)], piece_sem.at[m, at, lax.rem(group + g, groups)]

    sent = [0] * blocks

    def push(source, target, out_sem, in_sem, **where):
        pltpu.make_async_remote_copy(
            src_ref=source, dst_ref=target, send_sem=out_sem, recv_sem=in_sem, device_id=where, device_id_type=MESH
        ).start()

    def settle(like, sem):
        pltpu.make_async_copy(like, like, sem).wait()

    def settle_pieces(count, sem):
        total = count * piece
        if total <= width:
            settle(weights.at[0, pl.ds(0, total)], sem)
        else:
            settle(raw.at[pl.ds(0, total * span // width)], sem)

    def lead(step):
        if leads == 1:
            pl.when(leading)(step)
        else:
            step()

    def to_places(m, r, g):
        block, sem = piece_at(m, r, 0, g)
        for j in range(1, inner):
            push(block, block, send_sem.at[m // merged], sem, sp=lane * inner + lax.rem(place + j, inner))
            sent[m] += 1

    def to_groups(m, r, j):
        block, sem = piece_at(m, r, j, 0)
        for g in range(1, groups):
            push(block, block, send_sem.at[m // merged], sem, gr=lax.rem(group + g, groups))
            sent[m] += 1

    def to_sections(m, r, j, g):
        block, _ = piece_at(m, r, j, g)
        for t in range(1, sections):
            push(block, block, send_sem.at[m // merged], cross_sem.at[m, r], tp=lax.rem(section + t, sections))
            sent[m] += 1

    def outer(m):
        return depth == 4 and OUTER[m % len(OUTER)]

    def arrive(m, r, j, g):
        settle(*piece_at(m, r, j, g))

    def step_own(m, _):
        loads[m].wait()
        lead(lambda: send_own(m))

    def send_own(m):
        block, sem = piece_at(m, 0, 0, 0)

        @pl.when(lane > 0)
        def _():
            push(block, block, send_sem.at[m // merged], sem, sp=seat - inner)

        @pl.when(lane < depth - 1)
        def _():
            push(block, block, send_sem.at[m // merged], sem, sp=seat + inner)

        if outer(m):
            for g in range(1, groups):
                other, its_sem = piece_at(m, 0, 0, g)
                across = lane + 1 - 2 * lax.rem(lane, 2)
                push(other, other, send_sem.at[m // merged], its_sem, sp=across * inner + place)
        to_places(m, 0, 0)
        if CORNER[m % len(CORNER)][0] == "y":
            for g in range(1, groups):
                to_places(m, 0, g)

    def step_lane(m, r):
        arrive(m, r, 0, 0)
        block, sem = piece_at(m, r, 0, 0)
        above = (ranks[r] - lane + depth) // depth
        onward = lane + 1 - 2 * above

        @pl.when((onward >= 0) & (onward < depth))
        def _():
            push(block, block, send_sem.at[m // merged], sem, sp=onward * inner + place)

        to_places(m, r, 0)
        if not (outer(m) and r == 1):
            to_groups(m, r, 0)
        to_sections(m, r, 0, 0)

    def corner(m, r):
        return CORNER[m % len(CORNER)][min(r, len(CORNER[0]) - 1)]

    def step_group(m, r):
        for g in range(1, groups):
            arrive(m, r, 0, g)
            if corner(m, r) == "y":
                to_places(m, r, g)
            to_sections(m, r, 0, g)

    def step_place(m, r):
        for j in range(1, inner):
            arrive(m, r, j, 0)
            if corner(m, r) == "x":
                to_groups(m, r, j)
            to_sections(m, r, j, 0)

    def step_corner(m, r):
        for j in range(1, inner):
            for g in range(1, groups):
                arrive(m, r, j, g)
                to_sections(m, r, j, g)

    filled, begun = set(), set()

    def add(m, out):
        if m in begun:
            acc[m] += out
        else:
            acc[m] = out
            begun.add(m)

    def step_norm(i, _):
        if not filled:
            smalls[0].wait()
        stage = i * norm_rows // fill_rows
        if stage not in filled:
            fills[stage].wait()
            filled.add(stage)
        step = 32

        @pl.loop(0, norm_rows // step)
        def _(k):
            here = pl.ds(pl.multiple_of(i * norm_rows + k * step, step), step)
            x = raw[here, :].astype(jnp.float32)
            mean = jnp.mean(x, axis=1, keepdims=True)
            centred = x - mean
            var = jnp.mean(centred * centred, axis=1, keepdims=True)
            scale = gain[...].astype(jnp.float32).reshape(1, width)
            normed[here, :] = (centred * lax.rsqrt(var + epsilon) * scale).astype(jnp.bfloat16)

    def crossed(m, r):
        count = ((inner - 1) if r == 0 else inner) * groups * (sections - 1 if leads > 1 else 1)
        if count and sections > 1:
            if leads > 1:
                settle_pieces(count, cross_sem.at[m, r])
            else:
                pl.when(section != sections - 1)(lambda: settle_pieces(count, cross_sem.at[m, r]))

    def step_pair(k, r):
        crossed(2 * k, r)
        crossed(2 * k + 1, r)
        long = inner * shard
        start = pl.multiple_of(ranks[r] * long, long)
        both = jnp.concatenate([weights[2 * k, pl.ds(start, long), :], weights[2 * k + 1, pl.ds(start, long), :]], axis=1)
        out = jnp.dot(normed[:, pl.ds(start, long)], both, preferred_element_type=jnp.float32)
        for m in range(2):
            add(2 * k + m, out[:, m * span:(m + 1) * span].T)

    def step_times(m, r):
        crossed(m, r)
        long = inner * shard
        start = pl.multiple_of(ranks[r] * long, long)
        add(m, lax.dot_general(
            weights[m, pl.ds(start, long), :], normed[:, pl.ds(start, long)], (((0,), (1,)), ((), ())),
            preferred_element_type=jnp.float32,
        ))

    def step_trade(m, _):
        kind, part = m // per_kind, m % per_kind
        block = acc[m].T
        for seq in range(seqs):
            for i in range(per_block):
                cut = slice(i * head_size, (i + 1) * head_size)
                first = block[seq * sub:seq * sub + half, cut]
                second = block[seq * sub + half:(seq + 1) * sub, cut]
                outgoing[m, seq * per_block + i] = jnp.concatenate([first, second], axis=1).astype(jnp.bfloat16)
        for seq in range(seqs):
            for i in range(per_block):
                to = seq * kv_heads + part * per_block + i
                at = seq * per_block + i

                @pl.when(seat != to)
                def _():
                    push(outgoing.at[m, at], incoming.at[kind, seat], last_sem.at[0], last_sem.at[1 + kind], sp=to)

                @pl.when(seat == to)
                def _():
                    incoming[kind, to] = outgoing[m, at]

    pl.semaphore_wait(barrier, inner + groups + sections - 3 + (lane + depth - 1) // depth + (2 * depth - 2 - lane) // depth)
    calls = (step_norm, step_own, step_lane, step_group, step_place, step_corner, step_times, step_pair, step_trade)
    for which, m, r in plan(blocks, depth):
        with jax.named_scope(f"{calls[which].__name__}_{m}_{r}"):
            if HOP <= which <= EDGE:
                lead(lambda: calls[which](m, r))
            else:
                calls[which](m, r)

    for copy in smalls[1:]:
        copy.wait()
    query = queries[...].astype(jnp.float32)
    query = jnp.concatenate([query[:, g * head_size:(g + 1) * head_size] for g in range(heads)], axis=0)
    blank = jnp.zeros_like(query)
    query = jnp.concatenate(
        [jnp.concatenate([query, blank], axis=1), jnp.concatenate([blank, query], axis=1)], axis=0
    ).astype(jnp.bfloat16)
    mine = lax.broadcasted_iota(jnp.int32, (kv_heads, heads), 0) == lax.rem(seat, kv_heads)
    shift = jnp.sum(jnp.where(mine, head_shift[...], 0.0), axis=0, keepdims=True)
    eye = lax.broadcasted_iota(jnp.int32, (heads, heads), 0) == lax.broadcasted_iota(jnp.int32, (heads, heads), 1)
    shift = jnp.sum(jnp.where(eye, jnp.broadcast_to(shift, (heads, heads)), 0.0), axis=1, keepdims=True)
    later = (
        lax.broadcasted_iota(jnp.int32, (half, half), 0) > lax.broadcasted_iota(jnp.int32, (half, half), 1)
    ).astype(jnp.float32)

    with jax.named_scope("keys_in"):
        settle(incoming.at[0, pl.ds(0, seats - 1)], last_sem.at[1])
    trace = jax.named_scope("logits")
    trace.__enter__()
    keys = incoming[0].reshape(seats * half, 2 * head_size)
    logits = lax.dot_general(query, keys, (((1,), (1,)), ((), ())), preferred_element_type=jnp.float32)
    logits = logits * head_size ** (-0.5)
    betas, keeps = [], []
    for at in range(2 * seats):
        q, h = at // 2, at % 2
        z = logits[h * heads:(h + 1) * heads, q * half:(q + 1) * half]
        z = z + shift + key_shift[:, at * half:(at + 1) * half]
        tail = jnp.log1p(jnp.exp(-jnp.abs(z)))
        betas.append(jnp.minimum(z, 0.0) - tail)
        keeps.append(jnp.minimum(-z, 0.0) - tail)
    within = jnp.dot(
        jnp.concatenate(keeps, axis=0), later, preferred_element_type=jnp.float32, precision=lax.Precision.HIGHEST
    )
    running = jnp.zeros((heads, 1), jnp.float32)
    local = [None] * (2 * seats)
    for at in reversed(range(2 * seats)):
        local[at] = jnp.exp(betas[at] + within[at * heads:(at + 1) * heads] + running)
        running = running + jnp.sum(keeps[at], axis=1, keepdims=True)
    local = jnp.concatenate(
        [jnp.concatenate(local[0::2], axis=1), jnp.concatenate(local[1::2], axis=1)], axis=0
    ).astype(jnp.bfloat16)
    trace.__exit__(None, None, None)
    with jax.named_scope("values_in"):
        settle(incoming.at[1, pl.ds(0, seats - 1)], last_sem.at[2])
    trace = jax.named_scope("part")
    trace.__enter__()
    values = incoming[1].reshape(seats * half, 2 * head_size)
    part = jnp.dot(local, values, preferred_element_type=jnp.float32)
    part = part[:heads, :head_size] + part[heads:, head_size:]
    parts[section] = jnp.concatenate([part, jnp.broadcast_to(running, part.shape)], axis=1)
    for t in range(1, sections):
        push(parts.at[section], parts.at[section], last_sem.at[3], last_sem.at[4], tp=lax.rem(section + t, sections))
    trace.__exit__(None, None, None)
    trace = jax.named_scope("cache")
    trace.__enter__()
    for q in range(seats):
        for h in range(2):
            cut = slice(h * head_size, (h + 1) * head_size)
            start = (2 * q + h) * half
            cache[0, start:start + half, :] = jnp.concatenate([incoming[0, q][:, cut], incoming[1, q][:, cut]], axis=1)
    def drain():
        for pair in range(blocks // merged):
            both = range(merged * pair, merged * (pair + 1))
            for k in range(depth):
                count = sum(sent[m] + (k + 1) * (k < depth - 1) + (depth - k) * (k > 0) + (groups - 1) * outer(m) for m in both)
                pl.when(lane == k)(lambda count=count: settle_pieces(count, send_sem.at[pair]))

    lead(drain)
    settle(incoming.at[:, pl.ds(0, seats - 1)], last_sem.at[0])
    trace.__exit__(None, None, None)
    trace = jax.named_scope("parts_in")
    trace.__enter__()
    if sections > 1:
        settle(parts.at[pl.ds(0, sections - 1)], last_sem.at[3])
        settle(parts.at[pl.ds(0, sections - 1)], last_sem.at[4])
    total = jnp.zeros((heads, head_size), jnp.float32)
    carry = jnp.zeros((heads, head_size), jnp.float32)
    for t in reversed(range(sections)):
        total = total + jnp.exp(carry) * parts[t][:, :head_size]
        carry = carry + parts[t][:, head_size:]
    for g in range(heads):
        read[:, g * head_size:(g + 1) * head_size] = total[g:g + 1, :]
    trace.__exit__(None, None, None)


def hand_over(cache, read, cache_out, read_out, sem):
    first = pltpu.make_async_copy(cache, cache_out, sem.at[0])
    second = pltpu.make_async_copy(read, read_out, sem.at[1])
    first.start()
    second.start()
    first.wait()
    second.wait()


def local(grid, tokens, ln_gain, w_key, w_value, queries, head_shift, key_shift):
    depth, inner, groups, sections = grid
    seats = depth * inner
    seqs, _, sub, width = tokens.shape
    rows = seqs * sub
    columns = w_key.shape[1]
    kv_heads, heads = head_shift.shape
    head_size = columns // kv_heads
    blocks = 2 * columns // LANES
    vmem = pl.BlockSpec(memory_space=pltpu.VMEM)
    hbm = pl.BlockSpec(memory_space=pl.ANY)
    operands = (tokens.reshape(rows, width), ln_gain, w_key, w_value, queries, head_shift, key_shift)
    cache, read = pl.pallas_call(
        functools.partial(body, grid, head_size),
        out_shape=(
            jax.ShapeDtypeStruct((1, seats * sub, 2 * head_size), jnp.bfloat16),
            jax.ShapeDtypeStruct((1, heads * head_size), jnp.float32),
        ),
        in_specs=[hbm] * len(operands),
        out_specs=(vmem, vmem),
        scratch_shapes=[
            pltpu.VMEM((rows, width), jnp.bfloat16),
            pltpu.VMEM((rows, width), jnp.bfloat16),
            pltpu.VMEM((blocks, width, LANES), jnp.bfloat16),
            pltpu.VMEM((blocks, LANES, rows), jnp.float32),
            pltpu.VMEM((blocks, seqs * LANES // head_size, sub // 2, 2 * head_size), jnp.bfloat16),
            pltpu.VMEM((2, seats, sub // 2, 2 * head_size), jnp.bfloat16),
            pltpu.VMEM((sections, heads, 2 * head_size), jnp.float32),
            pltpu.VMEM(ln_gain.shape, ln_gain.dtype),
            pltpu.VMEM(queries.shape, queries.dtype),
            pltpu.VMEM(head_shift.shape, head_shift.dtype),
            pltpu.VMEM(key_shift.shape, key_shift.dtype),
            pltpu.SemaphoreType.DMA((blocks if sections > 2 else blocks // 2,)),
            pltpu.SemaphoreType.DMA((blocks, seats, groups)),
            pltpu.SemaphoreType.DMA((blocks, depth)),
            pltpu.SemaphoreType.DMA((5,)),
            pltpu.SemaphoreType.DMA((blocks + FILLS + 4,)),
        ],
        compiler_params=pltpu.CompilerParams(
            collective_id=0, has_side_effects=True, vmem_limit_bytes=24 * 1024 * 1024
        ),
    )(*(pltpu.with_memory_space_constraint(x, pltpu.HBM) for x in operands))
    return pl.pallas_call(
        hand_over,
        out_shape=(jax.ShapeDtypeStruct(cache.shape, cache.dtype), jax.ShapeDtypeStruct(read.shape, read.dtype)),
        in_specs=[vmem, vmem],
        out_specs=(hbm, hbm),
        scratch_shapes=[pltpu.SemaphoreType.DMA((2,))],
        compiler_params=pltpu.CompilerParams(vmem_limit_bytes=4 * 1024 * 1024),
    )(cache, read)


def solution(mesh):
    in_specs = (
        P("gr", "tp", "sp", None),
        P(),
        P("sp", None),
        P("sp", None),
        P(("gr", "sp"), None),
        P(),
        P(("gr", "sp"), "tp"),
    )
    out_specs = (P(("gr", "sp"), "tp", None), P(("gr", "sp"), None))
    return jax.shard_map(
        functools.partial(local, layout(mesh)), mesh=mesh, in_specs=in_specs, out_specs=out_specs, check_vma=False
    )
```
